32 devices in a mesh: sp: 16 (over z, y, x), tp: 2 (over core).
Axes of the slice: x: 2, y: 2, z: 4, core: 2. Of those that a mesh axis runs over, the one named last changes fastest.
Arguments:
- conv_out: bfloat16 [2048, 2048], P('sp', 'tp'), may hold values from -1500 to 1500
- ln_gain: float32 [2048], P('tp'), may hold values from 0.1 to 1.9
- taps: bfloat16 [31, 2048], P(None, 'tp'), may hold values from -1 to 1
- proj_weight: bfloat16 [2048, 2048], P('sp', 'tp'), may hold values from -0.125 to 0.125
- stream_mid: bfloat16 [2048, 2048], P('sp', 'tp'), may hold values from -6 to 6
- out_grad: bfloat16 [2048, 2048], P('sp', 'tp'), may hold values from -6 to 6
- routes: int32 [2048, 2], P('sp'), may hold values from 0 to 7, all different within a row; in each aligned block of 128 rows (0 to 127, 128 to 255, ...) at most 48 rows name the same one
- route_probs: float32 [2048, 2], P('sp'), may hold values from 0.2 to 1
- gate_slabs: bfloat16 [16, 2048, 1792], P('sp', None, 'tp'), may hold values from -0.125 to 0.125
- up_slabs: bfloat16 [16, 2048, 1792], P('sp', None, 'tp'), may hold values from -0.125 to 0.125
- down_slabs: bfloat16 [16, 1792, 2048], P('sp', 'tp'), may hold values from -0.09375 to 0.09375
Outputs:
- grad_input: bfloat16 [2048, 2048], P('sp', 'tp')
- grad_proj: float32 [2048, 2048], P('sp', 'tp')
- grad_gate: bfloat16 [16, 2048, 1792], P('sp', None, 'tp')
- grad_up: bfloat16 [16, 2048, 1792], P('sp', None, 'tp')
- grad_down: bfloat16 [16, 1792, 2048], P('sp', 'tp')
The draws below stay inside these ranges and needn't reach their ends.
Inputs may be any that keep to these rules, and one draw needn't show every extreme that they name: `routes`: each row names two different experts. Among the rows of one device no expert is named more than 48 times, and in every draw some device's rows name some expert exactly 48 times.
All inputs are finite; a program needn't handle non-finite values.
Results may differ from the reference program's by a relative error of at most 0.015.
Values may be sent and summed in bfloat16 or wider, within the bound.
A program may use at most 128 MiB of HBM per device.

```python
import math
import jax
import jax.numpy as jnp
import numpy as np
from jax import lax

D = 2048
EXP_HIDDEN = 3584
CONV_WIDTH = 31
TOK_DEV = 128
EXPERTS = 8
CAP = 48
TOKENS = 2048
N_SP = 16
N_TP = 2


def draw_conv_out(key, part):
    keys = jax.random.split(key, 3)
    columns = jnp.arange(D, dtype=jnp.float32)
    col_scale = jnp.exp(jax.random.uniform(keys[0], (D,), jnp.float32, 0.0, math.log(10.0))) * 3.0 ** (columns / D)
    row_scale = jnp.exp(jax.random.uniform(keys[1], (TOKENS, 1), jnp.float32, 0.0, math.log(10.0)))
    base = jnp.clip(jax.random.normal(keys[2], (TOKENS, D), jnp.float32), -5.0, 5.0)
    return (base * col_scale[None, :] * row_scale).astype(jnp.bfloat16)


def with_spikes(array, stream_key, source, target, parts, factor):
    owner, partner = [(jnp.arange(array.shape[axis_at]) // (array.shape[axis_at] // parts)).reshape([-1 if axis == axis_at else 1 for axis in range(array.ndim)]) for axis_at in (source, target)]
    chosen = jax.random.permutation(stream_key, parts)[partner]
    strong = (owner == chosen) | (owner == (partner + parts // 2) % parts)
    return jnp.where(strong, factor * array, array)


def steps_of(key, shape, shards, low, top_value):
    def one(dim, parts):
        draws = jax.random.uniform(jax.random.fold_in(jax.random.fold_in(key, 6), dim), (parts,), jnp.float32, low / len(shards), top_value / len(shards))
        return jnp.repeat(jnp.exp(draws), shape[dim] // parts).reshape((-1,) + (1,) * (len(shape) - dim - 1))

    loudness = one(*shards[0])
    for cut in shards[1:]:
        loudness = loudness * one(*cut)
    return loudness


def shared_out(own_key, own, number, rows, amount, top, most, skew):
    sequence = jax.random.permutation(own_key, amount)
    crowded, common = load_shares(amount, rows * top, most, skew, True), load_shares(amount, rows * top, most, skew, False)
    places = jnp.arange(amount)

    def named(tallies, offset_by):
        used = int((tallies > 0).sum())
        fixed = max(1, used // 4)
        passed = fixed + (places - fixed + offset_by * (used - fixed)) % max(1, amount - fixed)
        return jnp.zeros((amount,), jnp.int32).at[sequence[jnp.where(places < fixed, places, passed)]].set(jnp.asarray(tallies, jnp.int32))

    tallies = jnp.where(number % 4 == 0, named(crowded, number // 4), named(common, number - number // 4 - 1))
    mixed = jax.random.permutation(jax.random.fold_in(own, 3), amount)
    source_of, receiver = mixed[0:amount // 2 * 2:2], mixed[1:amount // 2 * 2:2]
    margin = jnp.minimum(tallies[source_of] - 1, most - tallies[receiver]) // 2
    margin = jnp.where((source_of == sequence[0]) | (receiver == sequence[0]) | (tallies[receiver] == 0), 0, jnp.maximum(margin, 0))
    passed = jax.random.randint(jax.random.fold_in(own, 4), (amount // 2,), 0, 1 << 20) % (margin + 1)
    tallies = tallies.at[source_of].add(-passed).at[receiver].add(passed)
    items = jnp.searchsorted(jnp.cumsum(tallies), jnp.arange(rows * top), side="right").astype(jnp.int32)
    table = items.reshape(top, rows).T
    table = table[jax.random.permutation(jax.random.fold_in(own, 1), rows)]
    offset_by = jax.random.randint(jax.random.fold_in(own, 2), (rows, 1), 0, top)
    return jnp.take_along_axis(table, (jnp.arange(top)[None, :] + offset_by) % top, axis=1)


def load_shares(count, total, bound, skew, full):
    weights = [(1 << 20) // math.isqrt(grade ** skew) + 1 for grade in range(1, count + 1)]
    largest = bound if full else min(bound, max(-(-total // count), total * weights[0] // sum(weights)))
    least = 1 if total - largest >= count - 1 else 0
    given, rest = [largest] + [least] * (count - 1), total - largest - least * (count - 1)
    while rest > 0:
        free = [i for i in range(1, count) if given[i] < largest] or [i for i in range(1, count) if given[i] < bound]
        pool, left = sum([weights[i] for i in free]), rest
        for i in free:
            more = min(bound - given[i], max(1, left * weights[i] // pool), rest)
            given[i] = given[i] + more
            rest = rest - more
    return np.array(given)


def scatter_about(key, extent, deviation, most, pieces=(), kind=jnp.bfloat16):
    array = deviation * jax.random.normal(key, extent, jnp.float32)
    if pieces:
        array = array * steps_of(key, extent, pieces, -0.22, 0.18)
    return jnp.clip(array, -most, most).astype(kind)


def gaussian_with(key, shape, width, most, shards, heavy, kind=jnp.bfloat16):
    values = width * jax.random.normal(key, shape, jnp.float32)
    if shards:
        values = values * steps_of(key, shape, shards, -0.22, 0.18)
    return jnp.clip(with_spikes(values, jax.random.fold_in(key, 3), *heavy), -most, most).astype(kind)


def setup_inputs(seed: int = 0) -> dict:
    splits = jax.random.split(jax.random.key(seed), 12)
    conv_out = draw_conv_out(jax.random.fold_in(splits[11], 71), 0)
    ln_gain = jnp.clip(1.0 + 0.18 * jax.random.normal(splits[1], (D,), jnp.float32), 0.1, 1.9)
    taps = scatter_about(splits[2], (CONV_WIDTH, D), CONV_WIDTH ** -0.5, 1.0, ((1, 2),))
    proj_weight = scatter_about(splits[3], (D, D), D ** -0.5, 0.125, ((0, 16), (1, 2)))
    stream_mid = scatter_about(splits[4], (TOKENS, D), 1.0, 6.0, ((0, 16), (1, 2)))
    out_grad = gaussian_with(splits[5], (TOKENS, D), 1.0, 6.0, ((0, 16), (1, 2)), (0, 1, 16, 2.0))
    routes_keys = jax.random.split(jax.random.fold_in(splits[6], 1), TOKENS // TOK_DEV)
    routes_turns = jax.random.permutation(jax.random.fold_in(splits[6], 3), TOKENS // TOK_DEV)
    routes = jax.vmap(lambda own, number: shared_out(jax.random.fold_in(splits[6], 2), own, number, TOK_DEV, EXPERTS, 2, CAP, 1))(routes_keys, routes_turns).reshape((TOKENS, 2))
    route_probs = jnp.clip(0.2 + 0.8 * jax.random.uniform(splits[7], (TOKENS, 2), jnp.float32) ** steps_of(splits[7], (TOKENS, 2), ((0, 16),), -0.2, 0.2), 0.2, 1.0)
    gate_slabs = scatter_about(splits[8], (2 * EXPERTS, D, EXP_HIDDEN // 2), D ** -0.5, 0.125, ((0, 16), (2, 2)))
    up_slabs = scatter_about(splits[9], (2 * EXPERTS, D, EXP_HIDDEN // 2), D ** -0.5, 0.125, ((0, 16), (2, 2)))
    down_slabs = scatter_about(splits[10], (2 * EXPERTS, EXP_HIDDEN // 2, D), EXP_HIDDEN ** -0.5, 0.09375, ((0, 16), (1, 2)))
    return {"conv_out": conv_out, "ln_gain": ln_gain, "taps": taps, "proj_weight": proj_weight, "stream_mid": stream_mid, "out_grad": out_grad, "routes": routes, "route_probs": route_probs, "gate_slabs": gate_slabs, "up_slabs": up_slabs, "down_slabs": down_slabs}


def dispatch_table(route_block, experts, capacity):
    tok_rows = route_block.shape[0]
    labels = jnp.arange(experts, dtype=jnp.int32)
    onehot = (route_block[:, :, None] == labels[None, None, :]).astype(jnp.float32)
    per_token = lax.optimization_barrier(jnp.sum(onehot, axis=1))
    earlier = (jnp.arange(tok_rows)[:, None] > jnp.arange(tok_rows)[None, :]).astype(jnp.float32)
    before = jnp.dot(earlier, per_token, precision=lax.Precision.HIGHEST)
    slot_index = lax.optimization_barrier(jnp.sum(onehot * before[:, None, :], axis=2)).astype(jnp.int32)
    position = route_block * capacity + slot_index
    columns = jnp.arange(experts * capacity, dtype=jnp.int32)
    first_pick = position[:, 0:1] == columns[None, :]
    second_pick = position[:, 1:2] == columns[None, :]
    return (first_pick, second_pick)

def half_grads(expert_in, expert_grad, weight, w_gate, w_up, w_down):
    gate_value = jnp.dot(expert_in, w_gate, preferred_element_type=jnp.float32)
    up_value = jnp.dot(expert_in, w_up, preferred_element_type=jnp.float32)
    gate_sig = jax.nn.sigmoid(gate_value)
    hidden_act = gate_value * gate_sig * up_value
    scaled = (weight[:, None] * hidden_act).astype(jnp.bfloat16)
    grad_down = jnp.dot(scaled.T, expert_grad, preferred_element_type=jnp.float32).astype(jnp.bfloat16)
    grad_hidden = weight[:, None] * jnp.dot(expert_grad, w_down.T, preferred_element_type=jnp.float32)
    grad_gate_pre = (grad_hidden * up_value * gate_sig * (1.0 + gate_value * (1.0 - gate_sig))).astype(jnp.bfloat16)
    grad_up_pre = (grad_hidden * gate_value * gate_sig).astype(jnp.bfloat16)
    grad_gate = jnp.dot(expert_in.T, grad_gate_pre, preferred_element_type=jnp.float32).astype(jnp.bfloat16)
    grad_up = jnp.dot(expert_in.T, grad_up_pre, preferred_element_type=jnp.float32).astype(jnp.bfloat16)
    quarter = w_gate.shape[1] // N_TP
    returned = jnp.zeros(expert_in.shape, jnp.float32)
    for core_index in range(N_TP):
        low_col = core_index * quarter
        high_col = low_col + quarter
        piece = jnp.dot(grad_gate_pre[:, low_col:high_col], w_gate[:, low_col:high_col].T, preferred_element_type=jnp.float32)
        piece = piece + jnp.dot(grad_up_pre[:, low_col:high_col], w_up[:, low_col:high_col].T, preferred_element_type=jnp.float32)
        rounded = lax.optimization_barrier(piece.astype(jnp.bfloat16))
        returned = returned + rounded.astype(jnp.float32)
    return (grad_gate, grad_up, grad_down, returned.astype(jnp.bfloat16))

def reference(conv_out, ln_gain, taps, proj_weight, stream_mid, out_grad, routes, route_probs, gate_slabs, up_slabs, down_slabs):
    slot_count = EXPERTS * CAP
    half_width = EXP_HIDDEN // 2

    def pack(inputs):
        route_block, mid_block, grad_block, prob_block = inputs
        first_pick, second_pick = dispatch_table(route_block, EXPERTS, CAP)
        route_table = (first_pick | second_pick).astype(jnp.float32)
        mid_slots = jnp.dot(route_table.T, mid_block.astype(jnp.float32), precision=lax.Precision.HIGHEST).astype(jnp.bfloat16)
        grad_slots = jnp.dot(route_table.T, grad_block.astype(jnp.float32), precision=lax.Precision.HIGHEST).astype(jnp.bfloat16)
        prob_slots = lax.optimization_barrier(jnp.sum(first_pick.astype(jnp.float32) * prob_block[:, 0:1] + second_pick.astype(jnp.float32) * prob_block[:, 1:2], axis=0))
        return (mid_slots, grad_slots, prob_slots)
    mid_slots, grad_slots, prob_slots = lax.map(pack, (routes.reshape(N_SP, TOK_DEV, 2), stream_mid.reshape(N_SP, TOK_DEV, D), out_grad.reshape(N_SP, TOK_DEV, D), route_probs.reshape(N_SP, TOK_DEV, 2)))

    def by_expert(slots):
        return slots.reshape(N_SP, EXPERTS, CAP, D).transpose(1, 0, 2, 3).reshape(EXPERTS, N_SP * CAP, D)
    probs_expert = prob_slots.reshape(N_SP, EXPERTS, CAP).transpose(1, 0, 2).reshape(EXPERTS, N_SP * CAP)

    def expert(inputs):
        expert_in, expert_grad, weight, gates, ups, downs = inputs
        first_half = half_grads(expert_in, expert_grad, weight, gates[0], ups[0], downs[0])
        second_half = half_grads(expert_in, expert_grad, weight, gates[1], ups[1], downs[1])
        return (jnp.stack([first_half[0], second_half[0]]), jnp.stack([first_half[1], second_half[1]]), jnp.stack([first_half[2], second_half[2]]), jnp.stack([first_half[3], second_half[3]]))
    grad_gate, grad_up, grad_down, returned = lax.map(expert, (by_expert(mid_slots), by_expert(grad_slots), probs_expert, gate_slabs.reshape(EXPERTS, 2, D, half_width), up_slabs.reshape(EXPERTS, 2, D, half_width), down_slabs.reshape(EXPERTS, 2, half_width, D)))
    returned = returned.reshape(EXPERTS, 2, N_SP, CAP, D).transpose(2, 0, 1, 3, 4)

    def unpack(inputs):
        route_block, back_rows, grad_block = inputs
        first_pick, second_pick = dispatch_table(route_block, EXPERTS, CAP)
        route_table = (first_pick | second_pick).astype(jnp.bfloat16)
        contrib = jnp.dot(route_table, back_rows[:, 0].reshape(slot_count, D), preferred_element_type=jnp.float32)
        contrib = contrib + jnp.dot(route_table, back_rows[:, 1].reshape(slot_count, D), preferred_element_type=jnp.float32)
        return (grad_block.astype(jnp.float32) + contrib).astype(jnp.bfloat16)
    grad_stream = lax.map(unpack, (routes.reshape(N_SP, TOK_DEV, 2), returned, out_grad.reshape(N_SP, TOK_DEV, D))).reshape(TOKENS, D)
    values = conv_out.astype(jnp.float32)
    row_mean = lax.optimization_barrier(jnp.mean(values, axis=1, keepdims=True))
    row_var = lax.optimization_barrier(jnp.mean(values * values, axis=1, keepdims=True)) - row_mean * row_mean
    inv_std = lax.rsqrt(row_var + 1e-06)
    normed = (values - row_mean) * inv_std
    scaled_z = normed * ln_gain[None, :]
    z_sig = jax.nn.sigmoid(scaled_z)
    activated = (scaled_z * z_sig).astype(jnp.bfloat16)
    grad_act = jnp.dot(grad_stream, proj_weight, preferred_element_type=jnp.float32)
    grad_normed = grad_act * z_sig * (1.0 + scaled_z * (1.0 - z_sig)) * ln_gain[None, :]
    first_mean = lax.optimization_barrier(jnp.mean(grad_normed, axis=1, keepdims=True))
    second_mean = lax.optimization_barrier(jnp.mean(grad_normed * normed, axis=1, keepdims=True))
    grad_conv = (inv_std * (grad_normed - first_mean - normed * second_mean)).astype(jnp.bfloat16)
    extended = jnp.concatenate([grad_conv, jnp.zeros((CONV_WIDTH - 1, D), jnp.bfloat16)], axis=0).astype(jnp.float32)
    tap_values = taps.astype(jnp.float32)
    grad_input = jnp.zeros((TOKENS, D), jnp.float32)
    for offset in range(CONV_WIDTH):
        grad_input = grad_input + tap_values[offset][None, :] * extended[offset:offset + TOKENS]
    grad_proj = jnp.dot(grad_stream.T, activated, preferred_element_type=jnp.float32)
    return (grad_input.astype(jnp.bfloat16), grad_proj, grad_gate.reshape(2 * EXPERTS, D, half_width), grad_up.reshape(2 * EXPERTS, D, half_width), grad_down.reshape(2 * EXPERTS, half_width, D))
```

```python
import functools

import jax
import jax.numpy as jnp
from jax import lax
from jax.experimental import pallas as pl
from jax.experimental.pallas import tpu as pltpu
from jax.sharding import PartitionSpec as P

MESH = pl.DeviceIdType.MESH
F32 = jnp.float32
BF16 = jnp.bfloat16
EPS = 1e-06


def flipped(index, mask):
    bit, result = 1, index
    while bit <= mask:
        if mask & bit:
            result = result + bit * (1 - 2 * lax.rem(lax.div(index, bit), 2))
        bit *= 2
    return result


def contract(left, right, left_dim, right_dim, precision=None):
    return lax.dot_general(
        left,
        right,
        (((left_dim,), (right_dim,)), ((), ())),
        preferred_element_type=F32,
        precision=precision,
    )


def identity(size, kind):
    across = lax.broadcasted_iota(jnp.int32, (size, size), 0)
    along = lax.broadcasted_iota(jnp.int32, (size, size), 1)
    return (across == along).astype(F32).astype(kind)


def layer_kernel(
    n,
    q,
    conv_ref,
    gain_ref,
    taps_ref,
    proj_ref,
    mid_ref,
    grad_ref,
    routes_ref,
    probs_ref,
    gate_hbm,
    up_hbm,
    down_hbm,
    out_input,
    out_proj,
    out_gate,
    out_up,
    out_down,
    w_gate,
    w_up,
    w_down,
    table,
    pack,
    rows,
    prob_pack,
    prob_all,
    before_ref,
    named_ref,
    weight_ref,
    g_ref,
    u_ref,
    h_ref,
    scaled_ref,
    dg_ref,
    du_ref,
    give,
    taken,
    half,
    pair_in,
    pair_sum,
    final,
    stage_up,
    stage_down,
    stat_out,
    stat_in,
    mean_ref,
    inv_ref,
    act_all,
    w_all,
    gs_own,
    gs_all,
    p_out,
    p_in,
    p_own,
    q_sum,
    q_out,
    q_in,
    gn_ref,
    stat2_out,
    stat2_in,
    ext_ref,
    ext_f32,
    taps_f32,
    load_sem,
    send_sem,
    recv_sem,
    pass_send,
    core_send,
    core_recv,
    prob_send,
    prob_recv,
    stat_sem,
    w_send,
    w_recv,
    act_send,
    act_recv,
    give_send,
    give_recv,
    pair_send,
    pair_recv,
    fin_send,
    fin_recv,
    gs_send,
    gs_recv,
    p_send,
    p_recv,
    q_send,
    q_recv,
    halo_sem,
    out_sem,
    local_sem,
):
    me, core = lax.axis_index("sp"), lax.axis_index("tp")
    other = 1 - core
    tok, width = mid_ref.shape
    experts, _, cap, _ = pack.shape
    depth = 2 * width
    nz = n // q
    own_rows = proj_ref.shape[0]
    mine = pl.ds(pl.multiple_of(core * width, 128), width)
    my_e, parity = lax.div(me, 2), lax.rem(me, 2)
    beside = flipped(me, 1)
    my_z, my_b = lax.div(me, q), lax.rem(me, q)

    def remote(src, dst, send, recv, where):
        return pltpu.make_async_remote_copy(
            src_ref=src,
            dst_ref=dst,
            send_sem=send,
            recv_sem=recv,
            device_id=where,
            device_id_type=MESH,
        )

    def in_square(step):
        return my_z * q + lax.rem(my_b + step, q)

    def in_line(step):
        return lax.rem(my_z + step, nz) * q + my_b

    loads = [
        pltpu.make_async_copy(source.at[0], held, load_sem.at[i])
        for i, (source, held) in enumerate(
            ((gate_hbm, w_gate), (up_hbm, w_up), (down_hbm, w_down))
        )
    ]
    for copy in loads:
        copy.start()

    barrier = pltpu.get_barrier_semaphore()
    for step in range(1, n):
        pl.semaphore_signal(
            barrier, inc=1, device_id=(lax.rem(me + step, n), core), device_id_type=MESH
        )
    for step in range(q):
        pl.semaphore_signal(
            barrier, inc=1, device_id=(in_square(step), other), device_id_type=MESH
        )

    eye_f32 = identity(tok, F32)
    route_rows = contract(
        routes_ref[...].astype(F32), eye_f32, 0, 0, lax.Precision.HIGHEST
    )
    first, second = route_rows[0:1, :], route_rows[1:2, :]
    labels = lax.broadcasted_iota(jnp.int32, (experts, tok), 0).astype(F32)
    named = ((labels == first) | (labels == second)).astype(F32)
    upper = (
        lax.broadcasted_iota(jnp.int32, (tok, tok), 0)
        < lax.broadcasted_iota(jnp.int32, (tok, tok), 1)
    ).astype(F32)
    before = jnp.dot(named.astype(BF16), upper.astype(BF16), preferred_element_type=F32)
    slot = lax.broadcasted_iota(jnp.int32, (cap, tok), 0).astype(F32)
    for e in range(experts):
        hit = (slot == before[e : e + 1, :]) & (named[e : e + 1, :] > 0.5)
        table[e] = hit.astype(F32).astype(BF16)
    before_ref[...] = before
    named_ref[...] = named
    flat_table = table[...].reshape(experts * cap, tok)
    for kind, source in enumerate((mid_ref, grad_ref)):
        filled = jnp.dot(flat_table, source[...], preferred_element_type=F32)
        pack[:, kind] = filled.astype(BF16).reshape(experts, cap, width)

    pl.semaphore_wait(barrier, n - 1 + q)

    def direct(step):
        target = flipped(me, step)
        return remote(
            pack.at[lax.div(target, 2)],
            rows.at[me, :, :, mine],
            send_sem.at[step // 2],
            recv_sem.at[me],
            (target, core),
        )

    def to_side(origin, source, index):
        return remote(
            source,
            rows.at[origin, :, :, mine],
            pass_send.at[index],
            recv_sem.at[origin],
            (beside, core),
        )

    def to_core(origin, source, index):
        return remote(
            source,
            rows.at[origin, :, :, mine],
            core_send.at[index],
            core_recv.at[origin],
            (me, other),
        )

    sent = [direct(step) for step in range(2, n, 2)]
    own_side = to_side(me, pack.at[my_e], 0)
    own_core = to_core(me, pack.at[my_e], 0)
    own_side.start()
    for copy in sent:
        copy.start()
    own_core.start()
    sent += [own_side, own_core]
    own_copy = pltpu.make_async_copy(pack.at[my_e], rows.at[me, :, :, mine], local_sem.at[0])
    own_copy.start()

    prob_rows = contract(probs_ref[...], eye_f32, 0, 0, lax.Precision.HIGHEST)
    slot_wide = lax.broadcasted_iota(jnp.int32, (128, tok), 0).astype(F32)

    def prob_step(e, carry):
        chosen = jnp.where(first == e.astype(F32), prob_rows[0:1, :], prob_rows[1:2, :])
        hit = (slot_wide == before_ref[pl.ds(e, 1), :]) & (named_ref[pl.ds(e, 1), :] > 0.5)
        prob_pack[e] = contract(
            jnp.broadcast_to(chosen, (8, tok)),
            hit.astype(F32),
            1,
            1,
            lax.Precision.HIGHEST,
        )
        return carry

    lax.fori_loop(0, experts, prob_step, 0)
    prob_all[me] = prob_pack[my_e]

    chunk = 16

    def stat_step(i, carry):
        at = pl.ds(pl.multiple_of(i * chunk, chunk), chunk)
        values = conv_ref[at, :].astype(F32)
        total = jnp.sum(values, axis=1, keepdims=True)
        squares = jnp.sum(values * values, axis=1, keepdims=True)
        stat_out[0, at, :] = jnp.broadcast_to(total, (chunk, 128))
        stat_out[1, at, :] = jnp.broadcast_to(squares, (chunk, 128))
        return carry

    lax.fori_loop(0, tok // chunk, stat_step, 0)
    stat_copy = remote(stat_out, stat_in, stat_sem.at[0], stat_sem.at[1], (me, other))
    stat_copy.start()
    for step in range(1, n):
        target = flipped(me, step)
        copy = remote(
            prob_pack.at[lax.div(target, 2)],
            prob_all.at[me],
            prob_send.at[step],
            prob_recv.at[me],
            (target, core),
        )
        copy.start()
        sent.append(copy)
    stat_copy.wait()

    def normed_of(at):
        values = conv_ref[at, :].astype(F32)
        return (values - mean_ref[at, 0:1]) * inv_ref[at, 0:1]

    def act_step(i, carry):
        at = pl.ds(pl.multiple_of(i * chunk, chunk), chunk)
        mean = (stat_out[0, at, :] + stat_in[0, at, :]) / depth
        var = (stat_out[1, at, :] + stat_in[1, at, :]) / depth - mean * mean
        mean_ref[at, :] = mean
        inv_ref[at, :] = lax.rsqrt(var + EPS)
        z = normed_of(at) * gain_ref[...]
        act_all[my_b, at, :] = (z * jax.nn.sigmoid(z)).astype(BF16)
        return carry

    lax.fori_loop(0, tok // chunk, act_step, 0)
    w_all[my_z] = proj_ref[...]
    taps_f32[0 : taps_ref.shape[0], :] = taps_ref[...].astype(F32)

    for step in range(2, n + 1, 2):
        if step < n:
            origin = flipped(me, step)
            remote(
                pack.at[0], rows.at[origin, :, :, mine], send_sem.at[0], recv_sem.at[origin], (beside, core)
            ).wait_recv()
            for copy in (
                to_side(origin, rows.at[origin, :, :, mine], step // 2),
                to_core(origin, rows.at[origin, :, :, mine], step),
            ):
                copy.start()
                sent.append(copy)
        origin = flipped(me, step - 1)
        remote(
            pack.at[0], rows.at[origin, :, :, mine], send_sem.at[0], recv_sem.at[origin], (beside, core)
        ).wait_recv()
        copy = to_core(origin, rows.at[origin, :, :, mine], step - 1)
        copy.start()
        sent.append(copy)

    for step in range(1, nz):
        copy = remote(
            proj_ref, w_all.at[my_z], w_send.at[step], w_recv.at[my_z], (in_line(step), core)
        )
        copy.start()
        sent.append(copy)
    for step in range(1, q):
        copy = remote(
            act_all.at[my_b],
            act_all.at[my_b],
            act_send.at[step],
            act_recv.at[my_b],
            (in_square(step), core),
        )
        copy.start()
        sent.append(copy)

    for step in range(1, n):
        origin = flipped(me, step)
        remote(
            prob_pack.at[0], prob_all.at[origin], prob_send.at[0], prob_recv.at[origin], (beside, core)
        ).wait_recv()
    columns = contract(prob_all[:, 0, :], identity(n, F32), 0, 0, lax.Precision.HIGHEST)
    for origin in range(n):
        weight_ref[origin] = jnp.broadcast_to(columns[0:cap, origin : origin + 1], (cap, 128))

    own_copy.wait()
    theirs = pl.ds(pl.multiple_of(other * width, 128), width)
    for step in range(n):
        origin = flipped(me, step)
        remote(
            pack.at[0], rows.at[origin, :, :, theirs], core_send.at[0], core_recv.at[origin], (me, other)
        ).wait_recv()
    for copy in loads:
        copy.wait()

    tiles = 2
    blocks = n // tiles
    tile_rows = blocks * cap
    hidden = w_gate.shape[1]

    def give_copy(tile):
        return remote(
            give.at[tile], taken.at[tile], give_send.at[tile], give_recv.at[tile], (me, other)
        )

    def expert_step(tile, carry):
        base = tile * blocks
        here = rows[pl.ds(base, blocks), 0].reshape(tile_rows, depth)
        g_ref[...] = jnp.dot(here, w_gate[...], preferred_element_type=F32)
        u_ref[...] = jnp.dot(here, w_up[...], preferred_element_type=F32)
        cotangent = rows[pl.ds(base, blocks), 1].reshape(tile_rows, depth)
        h_ref[...] = contract(cotangent, w_down[...], 1, 1)

        def pointwise(i, carry):
            at = pl.ds(pl.multiple_of(i * chunk, chunk), chunk)
            to = pl.ds(pl.multiple_of(tile * tile_rows + i * chunk, chunk), chunk)
            weight = weight_ref.reshape(n * cap, 128)[to, :]
            for lane in range(0, hidden, 128):
                lanes = slice(lane, lane + 128)
                gate, up = g_ref[at, lanes], u_ref[at, lanes]
                sig = jax.nn.sigmoid(gate)
                silu = gate * sig
                scaled_ref[to, lanes] = (weight * (silu * up)).astype(BF16)
                down = weight * h_ref[at, lanes]
                dg_ref[to, lanes] = (down * up * sig * (1.0 + gate * (1.0 - sig))).astype(BF16)
                du_ref[to, lanes] = (down * silu).astype(BF16)
            return carry

        lax.fori_loop(0, tile_rows // chunk, pointwise, 0)
        span = pl.ds(pl.multiple_of(tile * tile_rows, chunk), tile_rows)

        def back(which):
            part = pl.ds(pl.multiple_of(which * width, 128), width)
            return contract(dg_ref[span, :], w_gate[part, :], 1, 1) + contract(
                du_ref[span, :], w_up[part, :], 1, 1
            )

        give[tile] = back(other).astype(BF16).reshape(blocks, cap, width)
        give_copy(tile).start()
        half[pl.ds(base, blocks)] = back(core).astype(BF16).reshape(blocks, cap, width)
        return carry

    lax.fori_loop(0, tiles, expert_step, 0)

    def add_step(tile, carry):
        give_copy(tile).wait()
        at = pl.ds(tile * blocks, blocks)
        half[at] = (half[at].astype(F32) + taken[tile].astype(F32)).astype(BF16)
        return carry

    lax.fori_loop(0, tiles, add_step, 0)

    for step in range(n - 1, 0, -2):
        origin = flipped(me, step)
        index = lax.div(origin, 2)
        copy = remote(
            half.at[origin], pair_in.at[index], pair_send.at[index], pair_recv.at[index], (beside, core)
        )
        copy.start()
        sent.append(copy)

    span_up = stage_up.shape[2]
    steps_up = depth // span_up

    def up_copies(step, slot):
        at = pl.ds(pl.multiple_of(step * span_up, span_up), span_up)
        return (
            pltpu.make_async_copy(stage_up.at[slot, 0], out_gate.at[0, at, :], out_sem.at[0, slot]),
            pltpu.make_async_copy(stage_up.at[slot, 1], out_up.at[0, at, :], out_sem.at[1, slot]),
        )

    def up_step(step, carry):
        slot = lax.rem(step, 2)

        @pl.when(step >= 2)
        def _():
            for copy in up_copies(step - 2, slot):
                copy.wait()

        at = pl.ds(pl.multiple_of(step * span_up, 128), span_up)
        left = rows[:, 0, :, at].reshape(n * cap, span_up)
        stage_up[slot, 0] = contract(left, dg_ref[...], 0, 0).astype(BF16)
        stage_up[slot, 1] = contract(left, du_ref[...], 0, 0).astype(BF16)
        for copy in up_copies(step, slot):
            copy.start()
        return carry

    span_down = stage_down.shape[2]
    steps_down = depth // span_down

    def down_copy(step, slot):
        at = pl.ds(pl.multiple_of(step * span_down, span_down), span_down)
        return pltpu.make_async_copy(stage_down.at[slot], out_down.at[0, :, at], out_sem.at[2, slot])

    def down_step(step, carry):
        slot = lax.rem(step, 2)

        @pl.when(step >= 2)
        def _():
            down_copy(step - 2, slot).wait()

        at = pl.ds(pl.multiple_of(step * span_down, 128), span_down)
        right = rows[:, 1, :, at].reshape(n * cap, span_down)
        stage_down[slot] = contract(scaled_ref[...], right, 0, 0).astype(BF16)
        down_copy(step, slot).start()
        return carry

    def pair_step(step):
        origin = flipped(me, step)
        index = lax.div(origin, 2)
        remote(
            half.at[0], pair_in.at[index], pair_send.at[0], pair_recv.at[index], (beside, core)
        ).wait_recv()
        total = (half[origin].astype(F32) + pair_in[index].astype(F32)).astype(BF16)
        if step == 0:
            final[my_e] = total
        else:
            pair_sum[index] = total
            copy = remote(
                pair_sum.at[index], final.at[my_e], fin_send.at[index], fin_recv.at[my_e], (origin, core)
            )
            copy.start()
            sent.append(copy)

    pair_steps = list(range(n - 2, -1, -2))
    for i, step in enumerate(pair_steps):
        pair_step(step)
    lax.fori_loop(0, steps_up, up_step, 0)
    lax.fori_loop(0, steps_down, down_step, 0)
    for step in range(2, n, 2):
        index = lax.div(flipped(me, step), 2)
        remote(
            pair_sum.at[0], final.at[index], fin_send.at[0], fin_recv.at[index], (beside, core)
        ).wait_recv()

    gs_total = contract(final[...].reshape(experts * cap, width), flat_table, 0, 0)
    gs_total = gs_total + contract(grad_ref[...], identity(tok, BF16), 0, 0)
    gs_own[...] = gs_total.astype(BF16).reshape(gs_own.shape)

    part = pl.ds(core * (nz // 2), nz // 2)
    for step in range(q):
        peer = lax.rem(my_b + step, q)
        for flip in range(2):
            if step == 0 and flip == 0:
                continue
            copy = remote(
                gs_own.at[:, peer],
                gs_all.at[my_b, part],
                gs_send.at[step, flip],
                gs_recv.at[my_b, core],
                (my_z * q + peer, other if flip else core),
            )
            copy.start()
            sent.append(copy)
    gs_copy = pltpu.make_async_copy(gs_own.at[:, my_b], gs_all.at[my_b, part], local_sem.at[1])
    gs_copy.start()
    for step in range(1, nz):
        origin = lax.rem(my_z + step, nz)
        remote(
            proj_ref, w_all.at[origin], w_send.at[0], w_recv.at[origin], (beside, core)
        ).wait_recv()
    for step in range(1, q):
        origin = lax.rem(my_b + step, q)
        remote(
            act_all.at[origin], act_all.at[origin], act_send.at[0], act_recv.at[origin], (beside, core)
        ).wait_recv()
    gs_copy.wait()
    for step in range(q):
        origin = lax.rem(my_b + step, q)
        for flip in range(2):
            if step == 0 and flip == 0:
                continue
            source = other if flip else core
            remote(
                gs_own.at[:, 0],
                gs_all.at[origin, pl.ds(source * (nz // 2), nz // 2)],
                gs_send.at[0, 0],
                gs_recv.at[origin, source],
                (me, other),
            ).wait_recv()

    line_rows = nz * own_rows
    for b in range(q):
        product = jnp.dot(
            gs_all[b].reshape(line_rows, tok), act_all[b], preferred_element_type=F32
        ).reshape(nz, own_rows, width)
        q_sum[...] = product if b == 0 else q_sum[...] + product
    q_out[...] = q_sum[...].astype(BF16)
    for step in range(1, nz):
        target = lax.rem(my_z + step, nz)
        copy = remote(
            q_out.at[target], q_in.at[my_z], q_send.at[step], q_recv.at[my_z], (in_line(step), core)
        )
        copy.start()
        sent.append(copy)

    w_line = w_all[...].reshape(line_rows, width)
    for step in range(1, q):
        target = lax.rem(my_b + step, q)
        p_out[target] = contract(gs_all[target].reshape(line_rows, tok), w_line, 0, 0).astype(BF16)
        copy = remote(
            p_out.at[target], p_in.at[my_b], p_send.at[step], p_recv.at[my_b], (in_square(step), core)
        )
        copy.start()
        sent.append(copy)
    p_own[...] = contract(gs_all[my_b].reshape(line_rows, tok), w_line, 0, 0)
    for step in range(1, q):
        origin = lax.rem(my_b + step, q)
        remote(
            p_out.at[0], p_in.at[origin], p_send.at[0], p_recv.at[origin], (beside, core)
        ).wait_recv()

    def gn_step(i, carry):
        at = pl.ds(pl.multiple_of(i * chunk, chunk), chunk)
        grad_act = p_own[at, :]
        for step in range(1, q):
            grad_act = grad_act + p_in[lax.rem(my_b + step, q), at, :].astype(F32)
        normed = normed_of(at)
        z = normed * gain_ref[...]
        sig = jax.nn.sigmoid(z)
        gn = grad_act * sig * (1.0 + z * (1.0 - sig)) * gain_ref[...]
        gn_ref[at, :] = gn
        stat2_out[0, at, :] = jnp.broadcast_to(jnp.sum(gn, axis=1, keepdims=True), (chunk, 128))
        stat2_out[1, at, :] = jnp.broadcast_to(
            jnp.sum(gn * normed, axis=1, keepdims=True), (chunk, 128)
        )
        return carry

    lax.fori_loop(0, tok // chunk, gn_step, 0)
    stat2_copy = remote(stat2_out, stat2_in, stat_sem.at[2], stat_sem.at[3], (me, other))
    stat2_copy.start()
    stat2_copy.wait()

    def conv_grad_step(i, carry):
        at = pl.ds(pl.multiple_of(i * chunk, chunk), chunk)
        first_mean = (stat2_out[0, at, :] + stat2_in[0, at, :])[:, 0:1] / depth
        second_mean = (stat2_out[1, at, :] + stat2_in[1, at, :])[:, 0:1] / depth
        grad_conv = inv_ref[at, 0:1] * (gn_ref[at, :] - first_mean - normed_of(at) * second_mean)
        ext_ref[at, :] = grad_conv.astype(BF16)
        return carry

    lax.fori_loop(0, tok // chunk, conv_grad_step, 0)

    reach = ext_ref.shape[0] - tok
    previous = lax.rem(me + n - 1, n)
    halo = remote(
        ext_ref.at[pl.ds(0, reach)],
        ext_ref.at[pl.ds(tok, reach)],
        halo_sem.at[0],
        halo_sem.at[1],
        (previous, core),
    )
    halo.start()
    ext_f32[0:tok, :] = ext_ref[0:tok, :].astype(F32)
    halo.wait()
    after = ext_ref[tok : tok + reach, :].astype(F32)
    ext_f32[tok : tok + reach, :] = jnp.where(me == n - 1, 0.0, after)

    def conv_step(i, carry):
        lanes = pl.ds(pl.multiple_of(i * 128, 128), 128)
        total = jnp.zeros((tok, 128), F32)
        for k in range(taps_ref.shape[0]):
            total = total + taps_f32[k : k + 1, lanes] * ext_f32[k : k + tok, lanes]
        out_input[:, lanes] = total.astype(BF16)
        return carry

    lax.fori_loop(0, width // 128, conv_step, 0)

    for step in range(1, nz):
        origin = lax.rem(my_z + step, nz)
        remote(
            q_out.at[0], q_in.at[origin], q_send.at[0], q_recv.at[origin], (beside, core)
        ).wait_recv()
    proj_total = q_sum[my_z]
    for step in range(1, nz):
        proj_total = proj_total + q_in[lax.rem(my_z + step, nz)].astype(F32)
    out_proj[...] = proj_total

    for step in range(steps_up - 2, steps_up):
        for copy in up_copies(step, step % 2):
            copy.wait()
    for step in range(steps_down - 2, steps_down):
        down_copy(step, step % 2).wait()
    for copy in sent:
        copy.wait_send()


def on_device(
    conv_out,
    ln_gain,
    taps,
    proj_weight,
    stream_mid,
    out_grad,
    routes,
    route_probs,
    gate_slabs,
    up_slabs,
    down_slabs,
):
    n = lax.axis_size("sp")
    q = 1
    while q * q * 4 <= n:
        q *= 2
    nz = n // q
    tok, width = conv_out.shape
    experts = n // 2
    cap = -(-(3 * tok // experts) // 16) * 16
    own_rows = proj_weight.shape[0]
    hidden = gate_slabs.shape[2]
    slots = n * cap
    reach = -(-(taps.shape[0] - 1) // 16) * 16
    vmem, dma = pltpu.VMEM, pltpu.SemaphoreType.DMA
    near = pl.BlockSpec(memory_space=pltpu.VMEM)
    far = pl.BlockSpec(memory_space=pl.ANY)
    return pl.pallas_call(
        functools.partial(layer_kernel, n, q),
        out_shape=(
            jax.ShapeDtypeStruct((tok, width), BF16),
            jax.ShapeDtypeStruct((own_rows, width), F32),
            jax.ShapeDtypeStruct(gate_slabs.shape, BF16),
            jax.ShapeDtypeStruct(up_slabs.shape, BF16),
            jax.ShapeDtypeStruct(down_slabs.shape, BF16),
        ),
        in_specs=[near] * 8 + [far] * 3,
        out_specs=(near, near, far, far, far),
        scratch_shapes=[
            vmem(gate_slabs.shape[1:], BF16),
            vmem(up_slabs.shape[1:], BF16),
            vmem(down_slabs.shape[1:], BF16),
            vmem((experts, cap, tok), BF16),
            vmem((experts, 2, cap, width), BF16),
            vmem((n, 2, cap, 2 * width), BF16),
            vmem((experts, 8, 128), F32),
            vmem((n, 8, 128), F32),
            vmem((experts, tok), F32),
            vmem((experts, tok), F32),
            vmem((n, cap, 128), F32),
            vmem((slots // 2, hidden), F32),
            vmem((slots // 2, hidden), F32),
            vmem((slots // 2, hidden), F32),
            vmem((slots, hidden), BF16),
            vmem((slots, hidden), BF16),
            vmem((slots, hidden), BF16),
            vmem((2, n // 2, cap, width), BF16),
            vmem((2, n // 2, cap, width), BF16),
            vmem((n, cap, width), BF16),
            vmem((experts, cap, width), BF16),
            vmem((experts, cap, width), BF16),
            vmem((experts, cap, width), BF16),
            vmem((2, 2, 256, hidden), BF16),
            vmem((2, hidden, 512), BF16),
            vmem((2, tok, 128), F32),
            vmem((2, tok, 128), F32),
            vmem((tok, 128), F32),
            vmem((tok, 128), F32),
            vmem((q, tok, width), BF16),
            vmem((nz, own_rows, width), BF16),
            vmem((nz // 2, q, own_rows, tok), BF16),
            vmem((q, nz, own_rows, tok), BF16),
            vmem((q, tok, width), BF16),
            vmem((q, tok, width), BF16),
            vmem((tok, width), F32),
            vmem((nz, own_rows, width), F32),
            vmem((nz, own_rows, width), BF16),
            vmem((nz, own_rows, width), BF16),
            vmem((tok, width), F32),
            vmem((2, tok, 128), F32),
            vmem((2, tok, 128), F32),
            vmem((tok + reach, width), BF16),
            vmem((tok + reach, width), F32),
            vmem((-(-taps.shape[0] // 8) * 8, width), F32),
            dma((3,)),
            dma((n // 2,)),
            dma((n,)),
            dma((n // 2,)),
            dma((n,)),
            dma((n,)),
            dma((n,)),
            dma((n,)),
            dma((4,)),
            dma((nz,)),
            dma((nz,)),
            dma((q,)),
            dma((q,)),
            dma((2,)),
            dma((2,)),
            dma((experts,)),
            dma((experts,)),
            dma((experts,)),
            dma((experts,)),
            dma((q, 2)),
            dma((q, 2)),
            dma((q,)),
            dma((q,)),
            dma((nz,)),
            dma((nz,)),
            dma((2,)),
            dma((3, 2)),
            dma((2,)),
        ],
        compiler_params=pltpu.CompilerParams(
            collective_id=0, has_side_effects=True, vmem_limit_bytes=66 * 2**20 - 2**21
        ),
        cost_estimate=pl.CostEstimate(
            flops=16 * slots * 2 * width * hidden, bytes_accessed=60_000_000, transcendentals=0
        ),
    )(
        conv_out,
        ln_gain[None],
        taps,
        proj_weight,
        stream_mid,
        out_grad,
        routes,
        route_probs,
        gate_slabs,
        up_slabs,
        down_slabs,
    )


def solution(mesh):
    return jax.shard_map(
        on_device,
        mesh=mesh,
        in_specs=(
            P("sp", "tp"),
            P("tp"),
            P(None, "tp"),
            P("sp", "tp"),
            P("sp", "tp"),
            P("sp", "tp"),
            P("sp", None),
            P("sp", None),
            P("sp", None, "tp"),
            P("sp", None, "tp"),
            P("sp", "tp", None),
        ),
        out_specs=(
            P("sp", "tp"),
            P("sp", "tp"),
            P("sp", None, "tp"),
            P("sp", None, "tp"),
            P("sp", "tp", None),
        ),
        check_vma=False,
    )
```

```python
import functools

import jax
import jax.numpy as jnp
from jax import lax
from jax.experimental import pallas as pl
from jax.experimental.pallas import tpu as pltpu
from jax.sharding import PartitionSpec as P

MESH = pl.DeviceIdType.MESH
F32 = jnp.float32
BF16 = jnp.bfloat16
EPS = 1e-06
VMEM_BYTES = 64 * 2**20
CHUNKS = 4


def flipped(index, mask):
    bit, result = 1, index
    while bit <= mask:
        if mask & bit:
            result = result + bit * (1 - 2 * lax.rem(lax.div(index, bit), 2))
        bit *= 2
    return result


def contract(left, right, left_dim, right_dim, precision=None):
    return lax.dot_general(
        left,
        right,
        (((left_dim,), (right_dim,)), ((), ())),
        preferred_element_type=F32,
        precision=precision,
    )


def identity(size, kind):
    across = lax.broadcasted_iota(jnp.int32, (size, size), 0)
    along = lax.broadcasted_iota(jnp.int32, (size, size), 1)
    return (across == along).astype(F32).astype(kind)


def layer_kernel(
    n,
    q,
    conv_ref,
    gain_ref,
    proj_ref,
    mid_ref,
    grad_ref,
    routes_ref,
    probs_ref,
    gate_hbm,
    up_hbm,
    down_hbm,
    out_ext,
    out_proj,
    out_gate,
    out_up,
    out_down,
    w_gate,
    w_up,
    w_down,
    table,
    pack,
    rows,
    prob_pack,
    prob_all,
    before_ref,
    named_ref,
    weight_ref,
    g_ref,
    u_ref,
    h_ref,
    scaled_ref,
    dg_ref,
    du_ref,
    give,
    taken,
    half,
    pair_in,
    final,
    stage_up,
    stage_down,
    stat_out,
    stat_in,
    mean_ref,
    inv_ref,
    act_all,
    w_all,
    gs_own,
    gs_all,
    p_out,
    p_in,
    p_own,
    q_sum,
    q_out,
    q_in,
    q_near,
    gn_ref,
    ext_ref,
    load_sem,
    send_sem,
    recv_sem,
    pass_send,
    core_send,
    core_recv,
    prob_send,
    prob_recv,
    stat_sem,
    w_send,
    w_recv,
    act_send,
    act_recv,
    give_send,
    give_recv,
    pair_send,
    pair_recv,
    fin_send,
    fin_recv,
    gs_send,
    gs_recv,
    p_send,
    p_recv,
    q_send,
    q_recv,
    near_recv,
    halo_sem,
    out_sem,
    local_sem,
):
    opened = []

    def phase(name):
        if opened:
            opened.pop().__exit__(None, None, None)
        if name:
            opened.append(jax.named_scope(name))
            opened[-1].__enter__()

    me, core = lax.axis_index("sp"), lax.axis_index("tp")
    other = 1 - core
    tok, width = mid_ref.shape
    experts, _, cap, _ = pack.shape
    depth = 2 * width
    nz = n // q
    own_rows = proj_ref.shape[0]
    mine = pl.ds(pl.multiple_of(core * width, 128), width)
    my_e, parity = lax.div(me, 2), lax.rem(me, 2)
    beside = flipped(me, 1)
    my_z, my_b = lax.div(me, q), lax.rem(me, q)

    def remote(src, dst, send, recv, where):
        return pltpu.make_async_remote_copy(
            src_ref=src,
            dst_ref=dst,
            send_sem=send,
            recv_sem=recv,
            device_id=where,
            device_id_type=MESH,
        )

    def in_square(step):
        return my_z * q + lax.rem(my_b + step, q)

    def in_line(step):
        return lax.rem(my_z + step, nz) * q + my_b

    phase("a_pack")
    loads = [
        pltpu.make_async_copy(source.at[0], held, load_sem.at[i])
        for i, (source, held) in enumerate(
            ((gate_hbm, w_gate), (up_hbm, w_up), (down_hbm, w_down))
        )
    ]
    for copy in loads:
        copy.start()

    barrier = pltpu.get_barrier_semaphore()
    for step in range(1, n):
        pl.semaphore_signal(
            barrier, inc=1, device_id=(lax.rem(me + step, n), core), device_id_type=MESH
        )
    for step in range(q):
        pl.semaphore_signal(
            barrier, inc=1, device_id=(in_square(step), other), device_id_type=MESH
        )

    route_rows = routes_ref[...].astype(F32)
    first, second = route_rows[0:1, :], route_rows[1:2, :]
    labels = lax.broadcasted_iota(jnp.int32, (experts, tok), 0).astype(F32)
    named = ((labels == first) | (labels == second)).astype(F32)
    upper = (
        lax.broadcasted_iota(jnp.int32, (tok, tok), 0)
        < lax.broadcasted_iota(jnp.int32, (tok, tok), 1)
    ).astype(F32)
    before = jnp.dot(named.astype(BF16), upper.astype(BF16), preferred_element_type=F32)
    slot = lax.broadcasted_iota(jnp.int32, (cap, tok), 0).astype(F32)
    for e in range(experts):
        hit = (slot == before[e : e + 1, :]) & (named[e : e + 1, :] > 0.5)
        table[e] = hit.astype(F32).astype(BF16)
    before_ref[...] = before
    named_ref[...] = named
    flat_table = table[...].reshape(experts * cap, tok)
    for kind, source in enumerate((mid_ref, grad_ref)):
        filled = jnp.dot(flat_table, source[...], preferred_element_type=F32)
        pack[:, kind] = filled.astype(BF16).reshape(experts, cap, width)

    prob_rows = probs_ref[...]
    slot_wide = lax.broadcasted_iota(jnp.int32, (128, tok), 0).astype(F32)

    def prob_step(e, carry):
        chosen = jnp.where(first == lax.convert_element_type(e, F32), prob_rows[0:1, :], prob_rows[1:2, :])
        hit = (slot_wide == before_ref[pl.ds(e, 1), :]) & (named_ref[pl.ds(e, 1), :] > 0.5)
        prob_pack[e] = contract(
            jnp.broadcast_to(chosen, (8, tok)),
            hit.astype(F32),
            1,
            1,
            lax.Precision.HIGHEST,
        )
        return carry

    lax.fori_loop(0, experts, prob_step, 0, unroll=4)
    prob_all[me] = prob_pack[my_e]

    phase("b_barrier_send")
    pl.semaphore_wait(barrier, n - 1 + q)

    def direct(step, kind):
        target = flipped(me, step)
        return remote(
            pack.at[lax.div(target, 2), kind],
            rows.at[me, kind, :, mine],
            send_sem.at[kind, step // 2],
            recv_sem.at[kind, me],
            (target, core),
        )

    def to_side(origin, kind, source, index):
        return remote(
            source,
            rows.at[origin, kind, :, mine],
            pass_send.at[kind, index],
            recv_sem.at[kind, origin],
            (beside, core),
        )

    def to_core(origin, kind, source, index):
        return remote(
            source,
            rows.at[origin, kind, :, mine],
            core_send.at[kind, index],
            core_recv.at[kind, origin],
            (me, other),
        )

    sent = []

    def begin(copy):
        copy.start()
        sent.append(copy)

    for kind in range(2):
        begin(to_side(me, kind, pack.at[my_e, kind], 0))
    for step in range(1, n):
        target = flipped(me, step)
        begin(
            remote(
                prob_pack.at[lax.div(target, 2)],
                prob_all.at[me],
                prob_send.at[step],
                prob_recv.at[me],
                (target, core),
            )
        )
    for step in range(2, n, 2):
        for kind in range(2):
            begin(direct(step, kind))
    for kind in range(2):
        begin(to_core(me, kind, pack.at[my_e, kind], 0))
    own_copy = pltpu.make_async_copy(pack.at[my_e], rows.at[me, :, :, mine], local_sem.at[0])
    own_copy.start()

    phase("c_prob_norm")
    chunk = 16

    def stat_step(i, carry):
        at = pl.ds(pl.multiple_of(i * chunk, chunk), chunk)
        values = conv_ref[at, :].astype(F32)
        total = jnp.sum(values, axis=1, keepdims=True)
        squares = jnp.sum(values * values, axis=1, keepdims=True)
        stat_out[0, at, :] = jnp.broadcast_to(total, (chunk, 128))
        stat_out[1, at, :] = jnp.broadcast_to(squares, (chunk, 128))
        return carry

    lax.fori_loop(0, tok // chunk, stat_step, 0)
    stat_copy = remote(stat_out, stat_in, stat_sem.at[0], stat_sem.at[1], (me, other))
    stat_copy.start()
    def normed_of(at):
        values = conv_ref[at, :].astype(F32)
        return (values - mean_ref[at, 0:1]) * inv_ref[at, 0:1]

    def act_step(i, carry):
        at = pl.ds(pl.multiple_of(i * chunk, chunk), chunk)
        mean = (stat_out[0, at, :] + stat_in[0, at, :]) / depth
        var = (stat_out[1, at, :] + stat_in[1, at, :]) / depth - mean * mean
        mean_ref[at, :] = mean
        inv_ref[at, :] = lax.rsqrt(var + EPS)
        z = normed_of(at) * gain_ref[...]
        act_all[my_b, at, :] = (z * jax.nn.sigmoid(z)).astype(BF16)
        return carry

    def act_part():
        stat_copy.wait()
        lax.fori_loop(0, tok // chunk, act_step, 0)
        w_all[my_z] = proj_ref[...]
        for part in range(2, q, 2):
            begin(act_copy(my_b, part))

    def act_copy(origin, step):
        return remote(
            act_all.at[origin],
            act_all.at[origin],
            act_send.at[step, lax.rem(origin, 2)],
            act_recv.at[origin],
            (flipped(me, step), core),
        )

    def act_arrival(origin):
        remote(
            act_all.at[origin], act_all.at[origin], act_send.at[1, 0], act_recv.at[origin], (beside, core)
        ).wait_recv()

    def w_copy(origin, step):
        return remote(
            w_all.at[origin],
            w_all.at[origin],
            w_send.at[step, lax.div(origin, nz // 2)],
            w_recv.at[origin],
            (flipped(me, step * q), core),
        )

    def w_arrival(origin):
        remote(
            w_all.at[origin], w_all.at[origin], w_send.at[1, 0], w_recv.at[origin], (beside, core)
        ).wait_recv()

    def arrived(origin, kind):
        remote(
            pack.at[0, 0],
            rows.at[origin, kind, :, mine],
            send_sem.at[0, 0],
            recv_sem.at[kind, origin],
            (beside, core),
        ).wait_recv()

    def relay(step):
        phase("d_relay%02d" % step)
        origin = flipped(me, step)
        for kind in range(2):
            arrived(origin, kind)
            source = rows.at[origin, kind, :, mine]
            if step % 2 == 0:
                begin(to_side(origin, kind, source, step // 2))
            begin(to_core(origin, kind, source, step))

    tile_rows = q * cap
    hidden = w_gate.shape[1]
    theirs = pl.ds(pl.multiple_of(other * width, 128), width)

    def tile_base(tile):
        return flipped(my_z, tile) * q

    def tile_span(tile):
        return pl.ds(pl.multiple_of(tile_base(tile) * cap, chunk), tile_rows)

    def ready(tile):
        for step in range(tile * q, tile * q + q):
            origin = flipped(me, step)
            for kind in range(2):
                remote(
                    pack.at[0, 0],
                    rows.at[origin, kind, :, theirs],
                    core_send.at[0, 0],
                    core_recv.at[kind, origin],
                    (me, other),
                ).wait_recv()

    def prob_part():
        for step in range(1, n):
            origin = flipped(me, step)
            remote(
                prob_pack.at[0],
                prob_all.at[origin],
                prob_send.at[0],
                prob_recv.at[origin],
                (beside, core),
            ).wait_recv()
        columns = contract(prob_all[:, 0, :], identity(n, F32), 0, 0, lax.Precision.HIGHEST)
        for origin in range(n):
            weight_ref[origin] = jnp.broadcast_to(columns[0:cap, origin : origin + 1], (cap, 128))

    def front(tile):
        phase("g_front%d" % tile)
        ready(tile)
        at = pl.ds(tile_base(tile), q)
        here = rows[at, 0].reshape(tile_rows, depth)
        g_ref[...] = jnp.dot(here, w_gate[...], preferred_element_type=F32)
        u_ref[...] = jnp.dot(here, w_up[...], preferred_element_type=F32)
        cotangent = rows[at, 1].reshape(tile_rows, depth)
        h_ref[...] = contract(cotangent, w_down[...], 1, 1)
        first_row = tile_base(tile) * cap

        def pointwise(i, carry):
            at = pl.ds(pl.multiple_of(i * chunk, chunk), chunk)
            to = pl.ds(pl.multiple_of(first_row + i * chunk, chunk), chunk)
            weight = weight_ref.reshape(n * cap, 128)[to, :]
            for lane in range(0, hidden, 128):
                lanes = slice(lane, lane + 128)
                gate, up = g_ref[at, lanes], u_ref[at, lanes]
                sig = jax.nn.sigmoid(gate)
                silu = gate * sig
                scaled_ref[to, lanes] = (weight * (silu * up)).astype(BF16)
                down = weight * h_ref[at, lanes]
                dg_ref[to, lanes] = (down * up * sig * (1.0 + gate * (1.0 - sig))).astype(BF16)
                du_ref[to, lanes] = (down * silu).astype(BF16)
            return carry

        lax.fori_loop(0, tile_rows // chunk, pointwise, 0)

    def back(tile):
        phase("h_back%d" % tile)
        span = tile_span(tile)

        def product(which):
            part = pl.ds(pl.multiple_of(which * width, 128), width)
            total = contract(dg_ref[span, :], w_gate[part, :], 1, 1)
            total = total + contract(du_ref[span, :], w_up[part, :], 1, 1)
            return total.astype(BF16).reshape(q, cap, width)

        give[tile] = product(other)
        copy = remote(
            give.at[tile], taken.at[tile], give_send.at[tile], give_recv.at[tile], (me, other)
        )
        copy.start()
        kept = product(core)
        copy.wait()
        total = kept.astype(F32) + taken[tile].astype(F32)
        half[pl.ds(tile_base(tile), q)] = total.astype(BF16)

    def pair_send_tile(tile):
        for step in range(tile * q + 1, tile * q + q, 2):
            origin = flipped(me, step)
            index = lax.div(origin, 2)
            begin(
                remote(
                    half.at[origin],
                    pair_in.at[index],
                    pair_send.at[index],
                    pair_recv.at[index],
                    (beside, core),
                )
            )

    def pair_sum_tile(tile):
        phase("i_pair%d" % tile)
        for step in range(tile * q, tile * q + q, 2):
            origin = flipped(me, step)
            index = lax.div(origin, 2)
            remote(
                half.at[0], pair_in.at[index], pair_send.at[0], pair_recv.at[index], (beside, core)
            ).wait_recv()
            total = (half[origin].astype(F32) + pair_in[index].astype(F32)).astype(BF16)
            if step == 0:
                final[my_e] = total
            else:
                half[origin] = total
                begin(
                    remote(
                        half.at[origin],
                        final.at[my_e],
                        fin_send.at[index],
                        fin_recv.at[my_e],
                        (origin, core),
                    )
                )

    span_up = stage_up.shape[2]
    steps_up = depth // span_up

    def up_copies(step, slot):
        at = pl.ds(pl.multiple_of(step * span_up, span_up), span_up)
        return (
            pltpu.make_async_copy(stage_up.at[slot, 0], out_gate.at[0, at, :], out_sem.at[0, slot]),
            pltpu.make_async_copy(stage_up.at[slot, 1], out_up.at[0, at, :], out_sem.at[1, slot]),
        )

    def up_step(step, carry):
        slot = lax.rem(step, 2)

        @pl.when(step >= 2)
        def _():
            for copy in up_copies(step - 2, slot):
                copy.wait()

        at = pl.ds(pl.multiple_of(step * span_up, 128), span_up)
        left = rows[:, 0, :, at].reshape(n * cap, span_up)
        stage_up[slot, 0] = contract(left, dg_ref[...], 0, 0).astype(BF16)
        stage_up[slot, 1] = contract(left, du_ref[...], 0, 0).astype(BF16)
        for copy in up_copies(step, slot):
            copy.start()
        return carry

    span_down = stage_down.shape[2]
    steps_down = depth // span_down

    def down_copy(step, slot):
        at = pl.ds(pl.multiple_of(step * span_down, span_down), span_down)
        return pltpu.make_async_copy(stage_down.at[slot], out_down.at[0, :, at], out_sem.at[2, slot])

    def down_step(step, carry):
        slot = lax.rem(step, 2)

        @pl.when(step >= 2)
        def _():
            down_copy(step - 2, slot).wait()

        at = pl.ds(pl.multiple_of(step * span_down, 128), span_down)
        right = rows[:, 1, :, at].reshape(n * cap, span_down)
        stage_down[slot] = contract(scaled_ref[...], right, 0, 0).astype(BF16)
        down_copy(step, slot).start()
        return carry

    far_tile, last_tile = nz - 2, nz - 1
    near_tiles = list(range(nz - 2))

    def start_gathers():
        for part in range(1, nz // 2 + 1):
            begin(w_copy(my_z, part))

    work = {}

    def after(step, *actions):
        work.setdefault(min(step, n - 1), []).extend(actions)

    def before_tiles():
        phase("f_prob")
        prob_part()
        own_copy.wait()
        for copy in loads:
            copy.wait()

    after(1, act_part)
    after(2 * q, before_tiles)
    for tile in near_tiles:
        after(max((tile + 1) * q + 2, 2 * q), functools.partial(front, tile))
    for tile in near_tiles[:-1]:
        after(n - q, functools.partial(back, tile))
    after(n - 2, start_gathers, functools.partial(front, far_tile))
    after(n - 3, functools.partial(back, far_tile), functools.partial(pair_send_tile, far_tile))
    for tile in near_tiles[:-1]:
        after(n - 3, functools.partial(pair_send_tile, tile))

    order = []
    for step in range(2, n, 2):
        order += [step, step - 1]
    for step in order + [n - 1]:
        relay(step)
        for action in work.get(step, ()):
            action()
    front(last_tile)
    pair_sum_tile(far_tile)
    back(last_tile)
    pair_send_tile(last_tile)
    for tile in near_tiles[:-1]:
        pair_sum_tile(tile)
    back(near_tiles[-1])
    pair_send_tile(near_tiles[-1])
    begin(act_copy(my_b, 1))
    phase("j_wgrad0")
    lax.fori_loop(0, 2, up_step, 0)
    pair_sum_tile(last_tile)
    phase("j_wgrad1")
    lax.fori_loop(2, 5, up_step, 0)
    pair_sum_tile(near_tiles[-1])
    w_arrival(flipped(my_z, nz // 2))
    for part in range(1, nz // 2):
        begin(w_copy(flipped(my_z, nz // 2), part))
    phase("j_wgrad3")
    lax.fori_loop(5, steps_up, up_step, 0)
    act_arrival(flipped(my_b, 1))
    for part in range(2, q, 2):
        begin(act_copy(flipped(my_b, 1), part))
    phase("j_wgrad2")
    lax.fori_loop(0, steps_down, down_step, 0)
    phase("k_final_wait")
    for step in range(2, n, 2):
        index = lax.div(flipped(me, step), 2)
        remote(
            half.at[0], final.at[index], fin_send.at[0], fin_recv.at[index], (beside, core)
        ).wait_recv()

    phase("l_gs")
    gs_total = contract(final[...].reshape(experts * cap, width), flat_table, 0, 0)
    gs_total = gs_total + contract(grad_ref[...], identity(tok, BF16), 0, 0)
    gs_own[...] = gs_total.astype(BF16).reshape(gs_own.shape)

    part = pl.ds(core * (nz // 2), nz // 2)
    for step in range(1, q):
        peer = flipped(my_b, step)
        begin(
            remote(
                gs_own.at[:, peer],
                gs_all.at[my_b, part],
                gs_send.at[step, 0],
                gs_recv.at[my_b, core],
                (my_z * q + peer, core),
            )
        )
    gs_copy = pltpu.make_async_copy(gs_own.at[:, my_b], gs_all.at[my_b, part], local_sem.at[1])
    gs_copy.start()

    def gs_arrived(origin, source):
        remote(
            gs_own.at[:, 0],
            gs_all.at[origin, pl.ds(source * (nz // 2), nz // 2)],
            gs_send.at[0, 0],
            gs_recv.at[origin, source],
            (me, other),
        ).wait_recv()

    for step in range(q):
        origin = flipped(my_b, step)
        source = gs_own.at[:, my_b]
        if step:
            gs_arrived(origin, core)
            source = gs_all.at[origin, part]
        begin(
            remote(
                source,
                gs_all.at[origin, part],
                gs_send.at[step, 1],
                gs_recv.at[origin, core],
                (me, other),
            )
        )
    for step in range(1, nz):
        if step != nz // 2:
            w_arrival(flipped(my_z, step))
    for step in range(2, q):
        act_arrival(flipped(my_b, step))
    gs_copy.wait()
    for step in range(q):
        gs_arrived(flipped(my_b, step), other)

    phase("m_q")
    line_rows = nz * own_rows
    for b in range(q):
        product = jnp.dot(
            gs_all[b].reshape(line_rows, tok), act_all[b], preferred_element_type=F32
        ).reshape(nz, own_rows, width)
        q_sum[...] = product if b == 0 else q_sum[...] + product
    q_out[...] = q_sum[...].astype(BF16)
    for step in list(range(2, nz, 2)) + [0]:
        begin(
            remote(
                q_out.at[flipped(my_z, step + 1)],
                q_near.at[step // 2],
                q_send.at[step + 1],
                near_recv.at[step // 2],
                (flipped(me, q), core),
            )
        )

    def near_arrived(step):
        remote(
            q_out.at[0], q_near.at[step // 2], q_send.at[0], near_recv.at[step // 2], (beside, core)
        ).wait_recv()

    phase("n_p")
    w_line = w_all[...].reshape(line_rows, width)
    for step in range(1, q):
        target = lax.rem(my_b + step, q)
        p_out[target] = contract(gs_all[target].reshape(line_rows, tok), w_line, 0, 0).astype(BF16)
        copy = remote(
            p_out.at[target], p_in.at[my_b], p_send.at[step], p_recv.at[my_b], (in_square(step), core)
        )
        copy.start()
        sent.append(copy)
    p_own[...] = contract(gs_all[my_b].reshape(line_rows, tok), w_line, 0, 0)
    phase("n_q_on")
    for step in range(2, nz, 2):
        target = flipped(my_z, step)
        near_arrived(step)
        q_out[target] = (q_sum[target] + q_near[step // 2].astype(F32)).astype(BF16)
        begin(
            remote(
                q_out.at[target],
                q_in.at[my_z],
                q_send.at[step],
                q_recv.at[my_z],
                (flipped(me, step * q), core),
            )
        )
    phase("n_p_wait")
    for step in range(1, q):
        origin = lax.rem(my_b + step, q)
        remote(
            p_out.at[0], p_in.at[origin], p_send.at[0], p_recv.at[origin], (beside, core)
        ).wait_recv()

    phase("o_gn")
    def gn_step(i, carry):
        at = pl.ds(pl.multiple_of(i * chunk, chunk), chunk)
        grad_act = p_own[at, :]
        for step in range(1, q):
            grad_act = grad_act + p_in[lax.rem(my_b + step, q), at, :].astype(F32)
        normed = normed_of(at)
        z = normed * gain_ref[...]
        sig = jax.nn.sigmoid(z)
        gn = grad_act * sig * (1.0 + z * (1.0 - sig)) * gain_ref[...]
        gn_ref[at, :] = gn
        stat_out[0, at, :] = jnp.broadcast_to(jnp.sum(gn, axis=1, keepdims=True), (chunk, 128))
        stat_out[1, at, :] = jnp.broadcast_to(
            jnp.sum(gn * normed, axis=1, keepdims=True), (chunk, 128)
        )
        return carry

    lax.fori_loop(0, tok // chunk, gn_step, 0)
    stat2_copy = remote(stat_out, stat_in, stat_sem.at[2], stat_sem.at[3], (me, other))
    stat2_copy.start()
    stat2_copy.wait()

    phase("p_gc_halo")

    def conv_grad_step(i, carry):
        at = pl.ds(pl.multiple_of(i * chunk, chunk), chunk)
        first_mean = (stat_out[0, at, :] + stat_in[0, at, :])[:, 0:1] / depth
        second_mean = (stat_out[1, at, :] + stat_in[1, at, :])[:, 0:1] / depth
        grad_conv = inv_ref[at, 0:1] * (gn_ref[at, :] - first_mean - normed_of(at) * second_mean)
        ext_ref[at, :] = grad_conv.astype(BF16)
        return carry

    reach = ext_ref.shape[0] - tok
    previous = lax.rem(me + n - 1, n)
    halo = remote(
        ext_ref.at[pl.ds(0, reach)],
        ext_ref.at[pl.ds(tok, reach)],
        halo_sem.at[0],
        halo_sem.at[1],
        (previous, core),
    )
    lax.fori_loop(0, reach // chunk, conv_grad_step, 0)
    halo.start()
    lax.fori_loop(reach // chunk, tok // chunk, conv_grad_step, 0)

    out_ext[0:tok, :] = ext_ref[0:tok, :]
    phase("r_qwait")
    near_arrived(0)
    for step in range(2, nz, 2):
        origin = flipped(my_z, step)
        remote(
            q_out.at[0], q_in.at[origin], q_send.at[0], q_recv.at[origin], (beside, core)
        ).wait_recv()
    phase("r_halo_wait")
    halo.wait()
    after_rows = ext_ref[tok : tok + reach, :].astype(F32)
    out_ext[tok : tok + reach, :] = jnp.where(me == n - 1, 0.0, after_rows).astype(BF16)
    proj_total = q_sum[my_z] + q_near[0].astype(F32)
    for step in range(2, nz, 2):
        proj_total = proj_total + q_in[flipped(my_z, step)].astype(F32)
    out_proj[...] = proj_total

    phase("s_end")
    for step in range(steps_up - 2, steps_up):
        for copy in up_copies(step, step % 2):
            copy.wait()
    for step in range(steps_down - 2, steps_down):
        down_copy(step, step % 2).wait()
    for copy in sent:
        copy.wait_send()
    phase(None)


def finish_kernel(
    ext_hbm,
    taps_hbm,
    proj_hbm,
    gate_hbm,
    up_hbm,
    down_hbm,
    out_input,
    out_proj,
    out_gate,
    out_up,
    out_down,
    gate,
    up,
    down,
    ext,
    taps,
    proj,
    ext_f32,
    taps_f32,
    in_sem,
    out_sem,
    small_sem,
):
    small = [
        pltpu.make_async_copy(source, held, small_sem.at[i])
        for i, (source, held) in enumerate(((ext_hbm, ext), (taps_hbm, taps), (proj_hbm, proj)))
    ]
    for copy in small:
        copy.start()
    ins, outs = [], []
    for part in range(CHUNKS):
        for i, (source, held, result) in enumerate(
            ((gate_hbm, gate, out_gate), (up_hbm, up, out_up), (down_hbm, down, out_down))
        ):
            size = held.shape[0] // CHUNKS
            at = pl.ds(part * size, size)
            ins.append(pltpu.make_async_copy(source.at[0, at], held.at[at], in_sem.at[i, part]))
            outs.append(pltpu.make_async_copy(held.at[at], result.at[0, at], out_sem.at[i, part]))
    for copy in ins:
        copy.start()
    for copy in small:
        copy.wait()
    proj_copy = pltpu.make_async_copy(proj, out_proj, small_sem.at[3])
    proj_copy.start()
    taps_f32[...] = taps[...].astype(F32)
    tok, width = out_input.shape

    def conv_step(i, carry):
        lanes = pl.ds(pl.multiple_of(i * 128, 128), 128)
        ext_f32[:, lanes] = ext[:, lanes].astype(F32)
        total = jnp.zeros((tok, 128), F32)
        for k in range(taps.shape[0]):
            total = total + taps_f32[k : k + 1, lanes] * ext_f32[k : k + tok, lanes]
        out_input[:, lanes] = total.astype(BF16)
        return carry

    tiles = width // 128
    for part in range(CHUNKS):
        lax.fori_loop(part * tiles // CHUNKS, (part + 1) * tiles // CHUNKS, conv_step, 0)
        for copy_in, copy_out in zip(ins[3 * part : 3 * part + 3], outs[3 * part : 3 * part + 3]):
            copy_in.wait()
            copy_out.start()
    for copy in outs:
        copy.wait()
    proj_copy.wait()


def on_device(
    conv_out,
    ln_gain,
    taps,
    proj_weight,
    stream_mid,
    out_grad,
    routes,
    route_probs,
    gate_slabs,
    up_slabs,
    down_slabs,
):
    n = lax.axis_size("sp")
    q = 1
    while q * q * 4 <= n:
        q *= 2
    nz = n // q
    tok, width = conv_out.shape
    experts = n // 2
    cap = -(-(3 * tok // experts) // 16) * 16
    own_rows = proj_weight.shape[0]
    hidden = gate_slabs.shape[2]
    slots = n * cap
    reach = -(-(taps.shape[0] - 1) // 16) * 16
    vmem, dma = pltpu.VMEM, pltpu.SemaphoreType.DMA
    near = pl.BlockSpec(memory_space=pltpu.VMEM)
    far = pl.BlockSpec(memory_space=pl.ANY)
    buffers = [
        vmem(gate_slabs.shape[1:], BF16),
        vmem(up_slabs.shape[1:], BF16),
        vmem(down_slabs.shape[1:], BF16),
        vmem((experts, cap, tok), BF16),
        vmem((experts, 2, cap, width), BF16),
        vmem((n, 2, cap, 2 * width), BF16),
        vmem((experts, 8, 128), F32),
        vmem((n, 8, 128), F32),
        vmem((experts, tok), F32),
        vmem((experts, tok), F32),
        vmem((n, cap, 128), F32),
        vmem((q * cap, hidden), F32),
        vmem((q * cap, hidden), F32),
        vmem((q * cap, hidden), F32),
        vmem((slots, hidden), BF16),
        vmem((slots, hidden), BF16),
        vmem((slots, hidden), BF16),
        vmem((nz, q, cap, width), BF16),
        vmem((nz, q, cap, width), BF16),
        vmem((n, cap, width), BF16),
        vmem((experts, cap, width), BF16),
        vmem((experts, cap, width), BF16),
        vmem((2, 2, 256, hidden), BF16),
        vmem((2, hidden, 512), BF16),
        vmem((2, tok, 128), F32),
        vmem((2, tok, 128), F32),
        vmem((tok, 128), F32),
        vmem((tok, 128), F32),
        vmem((q, tok, width), BF16),
        vmem((nz, own_rows, width), BF16),
        vmem((nz // 2, q, own_rows, tok), BF16),
        vmem((q, nz, own_rows, tok), BF16),
        vmem((q, tok, width), BF16),
        vmem((q, tok, width), BF16),
        vmem((tok, width), F32),
        vmem((nz, own_rows, width), F32),
        vmem((nz, own_rows, width), BF16),
        vmem((nz, own_rows, width), BF16),
        vmem((nz // 2, own_rows, width), BF16),
        vmem((tok, width), F32),
        vmem((tok + reach, width), BF16),
    ]
    semaphores = [
        dma((3,)),
        dma((2, n // 2)),
        dma((2, n)),
        dma((2, n // 2)),
        dma((2, n)),
        dma((2, n)),
        dma((n,)),
        dma((n,)),
        dma((4,)),
        dma((nz, 2)),
        dma((nz,)),
        dma((q, 2)),
        dma((q,)),
        dma((nz,)),
        dma((nz,)),
        dma((experts,)),
        dma((experts,)),
        dma((experts,)),
        dma((experts,)),
        dma((q, 2)),
        dma((q, 2)),
        dma((q,)),
        dma((q,)),
        dma((nz,)),
        dma((nz,)),
        dma((nz // 2,)),
        dma((2,)),
        dma((3, 2)),
        dma((2,)),
    ]
    ext, proj, gate, up, down = pl.pallas_call(
        functools.partial(layer_kernel, n, q),
        out_shape=(
            jax.ShapeDtypeStruct((tok + reach, width), BF16),
            jax.ShapeDtypeStruct((own_rows, width), F32),
            jax.ShapeDtypeStruct(gate_slabs.shape, BF16),
            jax.ShapeDtypeStruct(up_slabs.shape, BF16),
            jax.ShapeDtypeStruct(down_slabs.shape, BF16),
        ),
        in_specs=[near] * 7 + [far] * 3,
        out_specs=(near, near, far, far, far),
        scratch_shapes=buffers + semaphores,
        compiler_params=pltpu.CompilerParams(
            collective_id=0, has_side_effects=True, vmem_limit_bytes=VMEM_BYTES
        ),
        cost_estimate=pl.CostEstimate(
            flops=16 * slots * 2 * width * hidden, bytes_accessed=60_000_000, transcendentals=0
        ),
    )(
        conv_out,
        ln_gain[None],
        proj_weight,
        stream_mid,
        out_grad,
        routes.T,
        route_probs.T,
        gate_slabs,
        up_slabs,
        down_slabs,
    )
    whole = [pltpu.VMEM(x.shape[1:], BF16) for x in (gate, up, down)]
    return pl.pallas_call(
        finish_kernel,
        out_shape=(
            jax.ShapeDtypeStruct((tok, width), BF16),
            jax.ShapeDtypeStruct(proj.shape, F32),
            jax.ShapeDtypeStruct(gate.shape, BF16),
            jax.ShapeDtypeStruct(up.shape, BF16),
            jax.ShapeDtypeStruct(down.shape, BF16),
        ),
        in_specs=[far] * 6,
        out_specs=(near, far, far, far, far),
        scratch_shapes=whole
        + [
            vmem(ext.shape, BF16),
            vmem(taps.shape, BF16),
            vmem(proj.shape, F32),
            vmem(ext.shape, F32),
            vmem(taps.shape, F32),
            dma((3, CHUNKS)),
            dma((3, CHUNKS)),
            dma((4,)),
        ],
        compiler_params=pltpu.CompilerParams(vmem_limit_bytes=VMEM_BYTES),
        cost_estimate=pl.CostEstimate(
            flops=2 * taps.shape[0] * tok * width, bytes_accessed=22_000_000, transcendentals=0
        ),
    )(ext, taps, proj, gate, up, down)


def solution(mesh):
    return jax.shard_map(
        on_device,
        mesh=mesh,
        in_specs=(
            P("sp", "tp"),
            P("tp"),
            P(None, "tp"),
            P("sp", "tp"),
            P("sp", "tp"),
            P("sp", "tp"),
            P("sp", None),
            P("sp", None),
            P("sp", None, "tp"),
            P("sp", None, "tp"),
            P("sp", "tp", None),
        ),
        out_specs=(
            P("sp", "tp"),
            P("sp", "tp"),
            P("sp", None, "tp"),
            P("sp", None, "tp"),
            P("sp", "tp", None),
        ),
        check_vma=False,
    )
```

```python
import functools

import jax
import jax.numpy as jnp
from jax import lax
from jax.experimental import pallas as pl
from jax.experimental.pallas import tpu as pltpu
from jax.sharding import PartitionSpec as P

MESH = pl.DeviceIdType.MESH
F32 = jnp.float32
BF16 = jnp.bfloat16
EPS = 1e-06
VMEM_BYTES = 64 * 2**20
CHUNKS = 4


def flipped(index, mask):
    bit, result = 1, index
    while bit <= mask:
        if mask & bit:
            result = result + bit * (1 - 2 * lax.rem(lax.div(index, bit), 2))
        bit *= 2
    return result


def contract(left, right, left_dim, right_dim, precision=None):
    return lax.dot_general(
        left,
        right,
        (((left_dim,), (right_dim,)), ((), ())),
        preferred_element_type=F32,
        precision=precision,
    )


def identity(size, kind):
    across = lax.broadcasted_iota(jnp.int32, (size, size), 0)
    along = lax.broadcasted_iota(jnp.int32, (size, size), 1)
    return (across == along).astype(F32).astype(kind)


def layer_kernel(
    n,
    q,
    conv_ref,
    gain_ref,
    proj_ref,
    mid_ref,
    grad_ref,
    routes_ref,
    probs_ref,
    gate_hbm,
    up_hbm,
    down_hbm,
    out_ext,
    out_proj,
    out_gate,
    out_up,
    out_down,
    w_gate,
    w_up,
    w_down,
    table,
    pack,
    rows,
    prob_pack,
    prob_all,
    before_ref,
    named_ref,
    weight_ref,
    g_ref,
    u_ref,
    h_ref,
    scaled_ref,
    dg_ref,
    du_ref,
    give,
    taken,
    half,
    pair_in,
    final,
    stage_up,
    stage_down,
    stat_out,
    stat_in,
    mean_ref,
    inv_ref,
    act_all,
    w_all,
    gs_own,
    gs_all,
    p_out,
    p_in,
    p_own,
    q_sum,
    q_out,
    q_in,
    q_near,
    gn_ref,
    ext_ref,
    load_sem,
    send_sem,
    recv_sem,
    pass_send,
    core_send,
    core_recv,
    prob_send,
    prob_recv,
    stat_sem,
    w_send,
    w_recv,
    act_send,
    act_recv,
    give_send,
    give_recv,
    pair_send,
    pair_recv,
    fin_send,
    fin_recv,
    gs_send,
    gs_recv,
    p_send,
    p_recv,
    q_send,
    q_recv,
    near_recv,
    halo_sem,
    out_sem,
    local_sem,
):
    opened = []

    def phase(name):
        if opened:
            opened.pop().__exit__(None, None, None)
        if name:
            opened.append(jax.named_scope(name))
            opened[-1].__enter__()

    me, core = lax.axis_index("sp"), lax.axis_index("tp")
    other = 1 - core
    tok, width = mid_ref.shape
    experts, _, cap, _ = pack.shape
    depth = 2 * width
    nz = n // q
    own_rows = proj_ref.shape[0]
    mine = pl.ds(pl.multiple_of(core * width, 128), width)
    my_e, parity = lax.div(me, 2), lax.rem(me, 2)
    beside = flipped(me, 1)
    my_z, my_b = lax.div(me, q), lax.rem(me, q)

    def remote(src, dst, send, recv, where):
        return pltpu.make_async_remote_copy(
            src_ref=src,
            dst_ref=dst,
            send_sem=send,
            recv_sem=recv,
            device_id=where,
            device_id_type=MESH,
        )

    def in_square(step):
        return my_z * q + lax.rem(my_b + step, q)

    def in_line(step):
        return lax.rem(my_z + step, nz) * q + my_b

    phase("a_pack")
    loads = [
        pltpu.make_async_copy(source.at[0], held, load_sem.at[i])
        for i, (source, held) in enumerate(
            ((gate_hbm, w_gate), (up_hbm, w_up), (down_hbm, w_down))
        )
    ]
    for copy in loads:
        copy.start()

    barrier = pltpu.get_barrier_semaphore()
    for step in range(1, n):
        pl.semaphore_signal(
            barrier, inc=1, device_id=(lax.rem(me + step, n), core), device_id_type=MESH
        )
    for step in range(q):
        pl.semaphore_signal(
            barrier, inc=1, device_id=(in_square(step), other), device_id_type=MESH
        )

    route_rows = routes_ref[...].astype(F32)
    first, second = route_rows[0:1, :], route_rows[1:2, :]
    labels = lax.broadcasted_iota(jnp.int32, (experts, tok), 0).astype(F32)
    named = ((labels == first) | (labels == second)).astype(F32)
    upper = (
        lax.broadcasted_iota(jnp.int32, (tok, tok), 0)
        < lax.broadcasted_iota(jnp.int32, (tok, tok), 1)
    ).astype(F32)
    before = jnp.dot(named.astype(BF16), upper.astype(BF16), preferred_element_type=F32)
    slot = lax.broadcasted_iota(jnp.int32, (cap, tok), 0).astype(F32)
    for e in range(experts):
        hit = (slot == before[e : e + 1, :]) & (named[e : e + 1, :] > 0.5)
        table[e] = hit.astype(F32).astype(BF16)
    before_ref[...] = before
    named_ref[...] = named
    flat_table = table[...].reshape(experts * cap, tok)
    for kind, source in enumerate((mid_ref, grad_ref)):
        filled = jnp.dot(flat_table, source[...], preferred_element_type=F32)
        pack[:, kind] = filled.astype(BF16).reshape(experts, cap, width)

    prob_rows = probs_ref[...]
    slot_wide = lax.broadcasted_iota(jnp.int32, (128, tok), 0).astype(F32)

    def prob_step(e, carry):
        chosen = jnp.where(first == lax.convert_element_type(e, F32), prob_rows[0:1, :], prob_rows[1:2, :])
        hit = (slot_wide == before_ref[pl.ds(e, 1), :]) & (named_ref[pl.ds(e, 1), :] > 0.5)
        prob_pack[e] = contract(
            jnp.broadcast_to(chosen, (8, tok)),
            hit.astype(F32),
            1,
            1,
            lax.Precision.HIGHEST,
        )
        return carry

    lax.fori_loop(0, experts, prob_step, 0, unroll=4)
    prob_all[me] = prob_pack[my_e]

    phase("b_barrier_send")
    pl.semaphore_wait(barrier, n - 1 + q)

    def direct(step, kind):
        target = flipped(me, step)
        return remote(
            pack.at[lax.div(target, 2), kind],
            rows.at[me, kind, :, mine],
            send_sem.at[kind, step // 2],
            recv_sem.at[kind, me],
            (target, core),
        )

    def to_side(origin, kind, source, index):
        return remote(
            source,
            rows.at[origin, kind, :, mine],
            pass_send.at[kind, index],
            recv_sem.at[kind, origin],
            (beside, core),
        )

    def to_core(origin, kind, source, index):
        return remote(
            source,
            rows.at[origin, kind, :, mine],
            core_send.at[kind, index],
            core_recv.at[kind, origin],
            (me, other),
        )

    sent = []

    def begin(copy):
        copy.start()
        sent.append(copy)

    for kind in range(2):
        begin(to_side(me, kind, pack.at[my_e, kind], 0))
    for step in range(1, n):
        target = flipped(me, step)
        begin(
            remote(
                prob_pack.at[lax.div(target, 2)],
                prob_all.at[me],
                prob_send.at[step],
                prob_recv.at[me],
                (target, core),
            )
        )
    for step in range(2, n, 2):
        for kind in range(2):
            begin(direct(step, kind))
    for kind in range(2):
        begin(to_core(me, kind, pack.at[my_e, kind], 0))
    own_copy = pltpu.make_async_copy(pack.at[my_e], rows.at[me, :, :, mine], local_sem.at[0])
    own_copy.start()

    phase("c_prob_norm")
    chunk = 16

    def stat_step(i, carry):
        at = pl.ds(pl.multiple_of(i * chunk, chunk), chunk)
        values = conv_ref[at, :].astype(F32)
        total = jnp.sum(values, axis=1, keepdims=True)
        squares = jnp.sum(values * values, axis=1, keepdims=True)
        stat_out[0, at, :] = jnp.broadcast_to(total, (chunk, 128))
        stat_out[1, at, :] = jnp.broadcast_to(squares, (chunk, 128))
        return carry

    lax.fori_loop(0, tok // chunk, stat_step, 0)
    stat_copy = remote(stat_out, stat_in, stat_sem.at[0], stat_sem.at[1], (me, other))
    stat_copy.start()
    def normed_of(at):
        values = conv_ref[at, :].astype(F32)
        return (values - mean_ref[at, 0:1]) * inv_ref[at, 0:1]

    def act_step(i, carry):
        at = pl.ds(pl.multiple_of(i * chunk, chunk), chunk)
        mean = (stat_out[0, at, :] + stat_in[0, at, :]) / depth
        var = (stat_out[1, at, :] + stat_in[1, at, :]) / depth - mean * mean
        mean_ref[at, :] = mean
        inv_ref[at, :] = lax.rsqrt(var + EPS)
        z = normed_of(at) * gain_ref[...]
        act_all[my_b, at, :] = (z * jax.nn.sigmoid(z)).astype(BF16)
        return carry

    def act_part():
        stat_copy.wait()
        lax.fori_loop(0, tok // chunk, act_step, 0)
        w_all[my_z] = proj_ref[...]
        begin(act_copy(my_b, 1))
        for part in range(2, q, 2):
            begin(act_copy(my_b, part))

    def act_copy(origin, step):
        return remote(
            act_all.at[origin],
            act_all.at[origin],
            act_send.at[step, lax.rem(origin, 2)],
            act_recv.at[origin],
            (flipped(me, step), core),
        )

    def act_arrival(origin):
        remote(
            act_all.at[origin], act_all.at[origin], act_send.at[1, 0], act_recv.at[origin], (beside, core)
        ).wait_recv()

    def w_copy(origin, step):
        return remote(
            w_all.at[origin],
            w_all.at[origin],
            w_send.at[step, lax.div(origin, nz // 2)],
            w_recv.at[origin],
            (flipped(me, step * q), core),
        )

    def w_arrival(origin):
        remote(
            w_all.at[origin], w_all.at[origin], w_send.at[1, 0], w_recv.at[origin], (beside, core)
        ).wait_recv()

    def arrived(origin, kind):
        remote(
            pack.at[0, 0],
            rows.at[origin, kind, :, mine],
            send_sem.at[0, 0],
            recv_sem.at[kind, origin],
            (beside, core),
        ).wait_recv()

    def relay(step):
        phase("d_relay%02d" % step)
        origin = flipped(me, step)
        for kind in range(2):
            arrived(origin, kind)
            source = rows.at[origin, kind, :, mine]
            if step % 2 == 0:
                begin(to_side(origin, kind, source, step // 2))
            begin(to_core(origin, kind, source, step))

    tile_rows = q * cap
    hidden = w_gate.shape[1]
    theirs = pl.ds(pl.multiple_of(other * width, 128), width)

    def tile_base(tile):
        return flipped(my_z, tile) * q

    def tile_span(tile):
        return pl.ds(pl.multiple_of(tile_base(tile) * cap, chunk), tile_rows)

    def ready(tile):
        for step in range(tile * q, tile * q + q):
            origin = flipped(me, step)
            for kind in range(2):
                remote(
                    pack.at[0, 0],
                    rows.at[origin, kind, :, theirs],
                    core_send.at[0, 0],
                    core_recv.at[kind, origin],
                    (me, other),
                ).wait_recv()

    def prob_part():
        for step in range(1, n):
            origin = flipped(me, step)
            remote(
                prob_pack.at[0],
                prob_all.at[origin],
                prob_send.at[0],
                prob_recv.at[origin],
                (beside, core),
            ).wait_recv()
        columns = contract(prob_all[:, 0, :], identity(n, F32), 0, 0, lax.Precision.HIGHEST)
        for origin in range(n):
            weight_ref[origin] = jnp.broadcast_to(columns[0:cap, origin : origin + 1], (cap, 128))

    def front(tile):
        phase("g_front%d" % tile)
        ready(tile)
        at = pl.ds(tile_base(tile), q)
        here = rows[at, 0].reshape(tile_rows, depth)
        g_ref[...] = jnp.dot(here, w_gate[...], preferred_element_type=F32)
        u_ref[...] = jnp.dot(here, w_up[...], preferred_element_type=F32)
        cotangent = rows[at, 1].reshape(tile_rows, depth)
        h_ref[...] = contract(cotangent, w_down[...], 1, 1)
        first_row = tile_base(tile) * cap

        def pointwise(i, carry):
            at = pl.ds(pl.multiple_of(i * chunk, chunk), chunk)
            to = pl.ds(pl.multiple_of(first_row + i * chunk, chunk), chunk)
            weight = weight_ref.reshape(n * cap, 128)[to, :]
            for lane in range(0, hidden, 128):
                lanes = slice(lane, lane + 128)
                gate, up = g_ref[at, lanes], u_ref[at, lanes]
                sig = jax.nn.sigmoid(gate)
                silu = gate * sig
                scaled_ref[to, lanes] = (weight * (silu * up)).astype(BF16)
                down = weight * h_ref[at, lanes]
                dg_ref[to, lanes] = (down * up * sig * (1.0 + gate * (1.0 - sig))).astype(BF16)
                du_ref[to, lanes] = (down * silu).astype(BF16)
            return carry

        lax.fori_loop(0, tile_rows // chunk, pointwise, 0)

    def back(tile):
        phase("h_back%d" % tile)
        span = tile_span(tile)

        def product(which):
            part = pl.ds(pl.multiple_of(which * width, 128), width)
            total = contract(dg_ref[span, :], w_gate[part, :], 1, 1)
            total = total + contract(du_ref[span, :], w_up[part, :], 1, 1)
            return total.astype(BF16).reshape(q, cap, width)

        give[tile] = product(other)
        copy = remote(
            give.at[tile], taken.at[tile], give_send.at[tile], give_recv.at[tile], (me, other)
        )
        copy.start()
        kept = product(core)
        copy.wait()
        total = kept.astype(F32) + taken[tile].astype(F32)
        half[pl.ds(tile_base(tile), q)] = total.astype(BF16)

    def pair_send_tile(tile):
        for step in range(tile * q + 1, tile * q + q, 2):
            origin = flipped(me, step)
            index = lax.div(origin, 2)
            begin(
                remote(
                    half.at[origin],
                    pair_in.at[index],
                    pair_send.at[index],
                    pair_recv.at[index],
                    (beside, core),
                )
            )

    def pair_sum_tile(tile):
        phase("i_pair%d" % tile)
        for step in range(tile * q, tile * q + q, 2):
            origin = flipped(me, step)
            index = lax.div(origin, 2)
            remote(
                half.at[0], pair_in.at[index], pair_send.at[0], pair_recv.at[index], (beside, core)
            ).wait_recv()
            total = (half[origin].astype(F32) + pair_in[index].astype(F32)).astype(BF16)
            if step == 0:
                final[my_e] = total
            else:
                half[origin] = total
                begin(
                    remote(
                        half.at[origin],
                        final.at[my_e],
                        fin_send.at[index],
                        fin_recv.at[my_e],
                        (origin, core),
                    )
                )

    span_up = stage_up.shape[2]
    steps_up = depth // span_up

    def up_copies(step, slot):
        at = pl.ds(pl.multiple_of(step * span_up, span_up), span_up)
        return (
            pltpu.make_async_copy(stage_up.at[slot, 0], out_gate.at[0, at, :], out_sem.at[0, slot]),
            pltpu.make_async_copy(stage_up.at[slot, 1], out_up.at[0, at, :], out_sem.at[1, slot]),
        )

    def up_step(step, carry):
        slot = lax.rem(step, 2)

        @pl.when(step >= 2)
        def _():
            for copy in up_copies(step - 2, slot):
                copy.wait()

        at = pl.ds(pl.multiple_of(step * span_up, 128), span_up)
        left = rows[:, 0, :, at].reshape(n * cap, span_up)
        stage_up[slot, 0] = contract(left, dg_ref[...], 0, 0).astype(BF16)
        stage_up[slot, 1] = contract(left, du_ref[...], 0, 0).astype(BF16)
        for copy in up_copies(step, slot):
            copy.start()
        return carry

    span_down = stage_down.shape[2]
    steps_down = depth // span_down

    def down_copy(step, slot):
        at = pl.ds(pl.multiple_of(step * span_down, span_down), span_down)
        return pltpu.make_async_copy(stage_down.at[slot], out_down.at[0, :, at], out_sem.at[2, slot])

    def down_step(step, carry):
        slot = lax.rem(step, 2)

        @pl.when(step >= 2)
        def _():
            down_copy(step - 2, slot).wait()

        at = pl.ds(pl.multiple_of(step * span_down, 128), span_down)
        right = rows[:, 1, :, at].reshape(n * cap, span_down)
        stage_down[slot] = contract(scaled_ref[...], right, 0, 0).astype(BF16)
        down_copy(step, slot).start()
        return carry

    far_tile, last_tile = nz - 2, nz - 1
    near_tiles = list(range(nz - 2))

    def start_gathers():
        for part in range(1, nz // 2 + 1):
            begin(w_copy(my_z, part))

    work = {}

    def after(step, *actions):
        work.setdefault(min(step, n - 1), []).extend(actions)

    def before_tiles():
        phase("f_prob")
        prob_part()
        own_copy.wait()
        for copy in loads:
            copy.wait()

    after(1, act_part)
    after(2 * q, before_tiles)
    for tile in near_tiles:
        after(max((tile + 1) * q + 2, 2 * q), functools.partial(front, tile))
    for tile in near_tiles[:-1]:
        after(n - q, functools.partial(back, tile))
    after(n - 2, start_gathers, functools.partial(front, far_tile))
    after(n - 3, functools.partial(back, far_tile), functools.partial(pair_send_tile, far_tile))
    for tile in near_tiles[:-1]:
        after(n - 3, functools.partial(pair_send_tile, tile))

    order = []
    for step in range(2, n, 2):
        order += [step, step - 1]
    for step in order + [n - 1]:
        relay(step)
        for action in work.get(step, ()):
            action()
    act_arrival(flipped(my_b, 1))
    for part in range(2, q, 2):
        begin(act_copy(flipped(my_b, 1), part))
    front(last_tile)
    pair_sum_tile(far_tile)
    back(last_tile)
    pair_send_tile(last_tile)
    for tile in near_tiles[:-1]:
        pair_sum_tile(tile)
    back(near_tiles[-1])
    pair_send_tile(near_tiles[-1])
    pair_sum_tile(last_tile)
    phase("j_wgrad1")
    lax.fori_loop(0, 5, up_step, 0)
    pair_sum_tile(near_tiles[-1])
    w_arrival(flipped(my_z, nz // 2))
    for part in range(1, nz // 2):
        begin(w_copy(flipped(my_z, nz // 2), part))
    phase("j_wgrad3")
    lax.fori_loop(5, steps_up, up_step, 0)
    phase("k_final_wait")
    for step in range(2, n, 2):
        index = lax.div(flipped(me, step), 2)
        remote(
            half.at[0], final.at[index], fin_send.at[0], fin_recv.at[index], (beside, core)
        ).wait_recv()

    phase("l_gs")
    gs_total = contract(final[...].reshape(experts * cap, width), flat_table, 0, 0)
    gs_total = gs_total + contract(grad_ref[...], identity(tok, BF16), 0, 0)
    gs_own[...] = gs_total.astype(BF16).reshape(gs_own.shape)

    part = pl.ds(core * (nz // 2), nz // 2)
    for step in range(1, q):
        peer = flipped(my_b, step)
        begin(
            remote(
                gs_own.at[:, peer],
                gs_all.at[my_b, part],
                gs_send.at[step, 0],
                gs_recv.at[my_b, core],
                (my_z * q + peer, core),
            )
        )
    gs_copy = pltpu.make_async_copy(gs_own.at[:, my_b], gs_all.at[my_b, part], local_sem.at[1])
    gs_copy.start()

    phase("l_gs_wait")

    def gs_arrived(origin, source):
        remote(
            gs_own.at[:, 0],
            gs_all.at[origin, pl.ds(source * (nz // 2), nz // 2)],
            gs_send.at[0, 0],
            gs_recv.at[origin, source],
            (me, other),
        ).wait_recv()

    for step in range(q):
        origin = flipped(my_b, step)
        source = gs_own.at[:, my_b]
        if step:
            gs_arrived(origin, core)
            source = gs_all.at[origin, part]
        begin(
            remote(
                source,
                gs_all.at[origin, part],
                gs_send.at[step, 1],
                gs_recv.at[origin, core],
                (me, other),
            )
        )
    for step in range(1, nz):
        if step != nz // 2:
            w_arrival(flipped(my_z, step))
    for step in range(2, q):
        act_arrival(flipped(my_b, step))
    gs_copy.wait()
    for step in range(q):
        gs_arrived(flipped(my_b, step), other)

    phase("m_q")
    line_rows = nz * own_rows
    for b in range(q):
        product = jnp.dot(
            gs_all[b].reshape(line_rows, tok), act_all[b], preferred_element_type=F32
        ).reshape(nz, own_rows, width)
        q_sum[...] = product if b == 0 else q_sum[...] + product
    q_out[...] = q_sum[...].astype(BF16)
    halves = [slice(0, width // 2), slice(width // 2, width)]
    for step in list(range(2, nz, 2)) + [0]:
        for i, columns in enumerate(halves):
            begin(
                remote(
                    q_out.at[flipped(my_z, step + 1), :, columns],
                    q_near.at[step // 2, :, columns],
                    q_send.at[step + 1, i],
                    near_recv.at[step // 2, i],
                    (flipped(me, q), core),
                )
            )

    def near_arrived(step, i):
        remote(
            q_out.at[0, :, halves[i]],
            q_near.at[step // 2, :, halves[i]],
            q_send.at[0, 0],
            near_recv.at[step // 2, i],
            (beside, core),
        ).wait_recv()

    def pass_on(i):
        columns = halves[i]
        for step in range(2, nz, 2):
            target = flipped(my_z, step)
            near_arrived(step, i)
            total = q_sum[target, :, columns] + q_near[step // 2, :, columns].astype(F32)
            q_out[target, :, columns] = total.astype(BF16)
            begin(
                remote(
                    q_out.at[target, :, columns],
                    q_in.at[my_z, :, columns],
                    q_send.at[step, i],
                    q_recv.at[my_z, i],
                    (flipped(me, step * q), core),
                )
            )

    phase("n_p")
    w_line = w_all[...].reshape(line_rows, width)
    for step in range(1, q):
        target = lax.rem(my_b + step, q)
        p_out[target] = contract(gs_all[target].reshape(line_rows, tok), w_line, 0, 0).astype(BF16)
        copy = remote(
            p_out.at[target], p_in.at[my_b], p_send.at[step], p_recv.at[my_b], (in_square(step), core)
        )
        copy.start()
        sent.append(copy)
    p_own[...] = contract(gs_all[my_b].reshape(line_rows, tok), w_line, 0, 0)
    phase("n_wgrad")
    lax.fori_loop(0, 1, down_step, 0)
    phase("n_q_on0")
    pass_on(0)
    phase("n_q_on1")
    lax.fori_loop(1, 2, down_step, 0)
    pass_on(1)
    phase("n_wgrad2")
    lax.fori_loop(2, steps_down, down_step, 0)
    phase("n_p_wait")
    for step in range(1, q):
        origin = lax.rem(my_b + step, q)
        remote(
            p_out.at[0], p_in.at[origin], p_send.at[0], p_recv.at[origin], (beside, core)
        ).wait_recv()

    phase("o_gn")
    def gn_step(i, carry):
        at = pl.ds(pl.multiple_of(i * chunk, chunk), chunk)
        grad_act = p_own[at, :]
        for step in range(1, q):
            grad_act = grad_act + p_in[lax.rem(my_b + step, q), at, :].astype(F32)
        normed = normed_of(at)
        z = normed * gain_ref[...]
        sig = jax.nn.sigmoid(z)
        gn = grad_act * sig * (1.0 + z * (1.0 - sig)) * gain_ref[...]
        gn_ref[at, :] = gn
        stat_out[0, at, :] = jnp.broadcast_to(jnp.sum(gn, axis=1, keepdims=True), (chunk, 128))
        stat_out[1, at, :] = jnp.broadcast_to(
            jnp.sum(gn * normed, axis=1, keepdims=True), (chunk, 128)
        )
        return carry

    lax.fori_loop(0, tok // chunk, gn_step, 0)
    stat2_copy = remote(stat_out, stat_in, stat_sem.at[2], stat_sem.at[3], (me, other))
    stat2_copy.start()
    stat2_copy.wait()

    phase("p_gc_halo")

    def conv_grad_step(i, carry):
        at = pl.ds(pl.multiple_of(i * chunk, chunk), chunk)
        first_mean = (stat_out[0, at, :] + stat_in[0, at, :])[:, 0:1] / depth
        second_mean = (stat_out[1, at, :] + stat_in[1, at, :])[:, 0:1] / depth
        grad_conv = inv_ref[at, 0:1] * (gn_ref[at, :] - first_mean - normed_of(at) * second_mean)
        ext_ref[at, :] = grad_conv.astype(BF16)
        return carry

    reach = ext_ref.shape[0] - tok
    previous = lax.rem(me + n - 1, n)
    halo = remote(
        ext_ref.at[pl.ds(0, reach)],
        ext_ref.at[pl.ds(tok, reach)],
        halo_sem.at[0],
        halo_sem.at[1],
        (previous, core),
    )
    lax.fori_loop(0, reach // chunk, conv_grad_step, 0)
    halo.start()
    lax.fori_loop(reach // chunk, tok // chunk, conv_grad_step, 0)

    out_ext[0:tok, :] = ext_ref[0:tok, :]
    phase("r_qwait")
    for i, columns in enumerate(halves):
        near_arrived(0, i)
        for step in range(2, nz, 2):
            origin = flipped(my_z, step)
            remote(
                q_out.at[0, :, columns],
                q_in.at[origin, :, columns],
                q_send.at[0, 0],
                q_recv.at[origin, i],
                (beside, core),
            ).wait_recv()
    phase("r_halo_wait")
    halo.wait()
    after_rows = ext_ref[tok : tok + reach, :].astype(F32)
    out_ext[tok : tok + reach, :] = jnp.where(me == n - 1, 0.0, after_rows).astype(BF16)
    proj_total = q_sum[my_z] + q_near[0].astype(F32)
    for step in range(2, nz, 2):
        proj_total = proj_total + q_in[flipped(my_z, step)].astype(F32)
    out_proj[...] = proj_total

    phase("s_end")
    for step in range(steps_up - 2, steps_up):
        for copy in up_copies(step, step % 2):
            copy.wait()
    for step in range(steps_down - 2, steps_down):
        down_copy(step, step % 2).wait()
    for copy in sent:
        copy.wait_send()
    phase(None)


def finish_kernel(
    ext_hbm,
    taps_hbm,
    proj_hbm,
    gate_hbm,
    up_hbm,
    down_hbm,
    out_input,
    out_proj,
    out_gate,
    out_up,
    out_down,
    gate,
    up,
    down,
    ext,
    taps,
    proj,
    ext_f32,
    taps_f32,
    in_sem,
    out_sem,
    small_sem,
):
    small = [
        pltpu.make_async_copy(source, held, small_sem.at[i])
        for i, (source, held) in enumerate(((ext_hbm, ext), (taps_hbm, taps), (proj_hbm, proj)))
    ]
    for copy in small:
        copy.start()
    ins, outs = [], []
    for part in range(CHUNKS):
        for i, (source, held, result) in enumerate(
            ((gate_hbm, gate, out_gate), (up_hbm, up, out_up), (down_hbm, down, out_down))
        ):
            size = held.shape[0] // CHUNKS
            at = pl.ds(part * size, size)
            ins.append(pltpu.make_async_copy(source.at[0, at], held.at[at], in_sem.at[i, part]))
            outs.append(pltpu.make_async_copy(held.at[at], result.at[0, at], out_sem.at[i, part]))
    for copy in ins:
        copy.start()
    for copy in small:
        copy.wait()
    proj_copy = pltpu.make_async_copy(proj, out_proj, small_sem.at[3])
    proj_copy.start()
    taps_f32[...] = taps[...].astype(F32)
    tok, width = out_input.shape

    def conv_step(i, carry):
        lanes = pl.ds(pl.multiple_of(i * 128, 128), 128)
        ext_f32[:, lanes] = ext[:, lanes].astype(F32)
        total = jnp.zeros((tok, 128), F32)
        for k in range(taps.shape[0]):
            total = total + taps_f32[k : k + 1, lanes] * ext_f32[k : k + tok, lanes]
        out_input[:, lanes] = total.astype(BF16)
        return carry

    tiles = width // 128
    for part in range(CHUNKS):
        lax.fori_loop(part * tiles // CHUNKS, (part + 1) * tiles // CHUNKS, conv_step, 0)
        for copy_in, copy_out in zip(ins[3 * part : 3 * part + 3], outs[3 * part : 3 * part + 3]):
            copy_in.wait()
            copy_out.start()
    for copy in outs:
        copy.wait()
    proj_copy.wait()


def on_device(
    conv_out,
    ln_gain,
    taps,
    proj_weight,
    stream_mid,
    out_grad,
    routes,
    route_probs,
    gate_slabs,
    up_slabs,
    down_slabs,
):
    n = lax.axis_size("sp")
    q = 1
    while q * q * 4 <= n:
        q *= 2
    nz = n // q
    tok, width = conv_out.shape
    experts = n // 2
    cap = -(-(3 * tok // experts) // 16) * 16
    own_rows = proj_weight.shape[0]
    hidden = gate_slabs.shape[2]
    slots = n * cap
    reach = -(-(taps.shape[0] - 1) // 16) * 16
    vmem, dma = pltpu.VMEM, pltpu.SemaphoreType.DMA
    near = pl.BlockSpec(memory_space=pltpu.VMEM)
    far = pl.BlockSpec(memory_space=pl.ANY)
    buffers = [
        vmem(gate_slabs.shape[1:], BF16),
        vmem(up_slabs.shape[1:], BF16),
        vmem(down_slabs.shape[1:], BF16),
        vmem((experts, cap, tok), BF16),
        vmem((experts, 2, cap, width), BF16),
        vmem((n, 2, cap, 2 * width), BF16),
        vmem((experts, 8, 128), F32),
        vmem((n, 8, 128), F32),
        vmem((experts, tok), F32),
        vmem((experts, tok), F32),
        vmem((n, cap, 128), F32),
        vmem((q * cap, hidden), F32),
        vmem((q * cap, hidden), F32),
        vmem((q * cap, hidden), F32),
        vmem((slots, hidden), BF16),
        vmem((slots, hidden), BF16),
        vmem((slots, hidden), BF16),
        vmem((nz, q, cap, width), BF16),
        vmem((nz, q, cap, width), BF16),
        vmem((n, cap, width), BF16),
        vmem((experts, cap, width), BF16),
        vmem((experts, cap, width), BF16),
        vmem((2, 2, 256, hidden), BF16),
        vmem((2, hidden, 512), BF16),
        vmem((2, tok, 128), F32),
        vmem((2, tok, 128), F32),
        vmem((tok, 128), F32),
        vmem((tok, 128), F32),
        vmem((q, tok, width), BF16),
        vmem((nz, own_rows, width), BF16),
        vmem((nz // 2, q, own_rows, tok), BF16),
        vmem((q, nz, own_rows, tok), BF16),
        vmem((q, tok, width), BF16),
        vmem((q, tok, width), BF16),
        vmem((tok, width), F32),
        vmem((nz, own_rows, width), F32),
        vmem((nz, own_rows, width), BF16),
        vmem((nz, own_rows, width), BF16),
        vmem((nz // 2, own_rows, width), BF16),
        vmem((tok, width), F32),
        vmem((tok + reach, width), BF16),
    ]
    semaphores = [
        dma((3,)),
        dma((2, n // 2)),
        dma((2, n)),
        dma((2, n // 2)),
        dma((2, n)),
        dma((2, n)),
        dma((n,)),
        dma((n,)),
        dma((4,)),
        dma((nz, 2)),
        dma((nz,)),
        dma((q, 2)),
        dma((q,)),
        dma((nz,)),
        dma((nz,)),
        dma((experts,)),
        dma((experts,)),
        dma((experts,)),
        dma((experts,)),
        dma((q, 2)),
        dma((q, 2)),
        dma((q,)),
        dma((q,)),
        dma((nz, 2)),
        dma((nz, 2)),
        dma((nz // 2, 2)),
        dma((2,)),
        dma((3, 2)),
        dma((2,)),
    ]
    ext, proj, gate, up, down = pl.pallas_call(
        functools.partial(layer_kernel, n, q),
        out_shape=(
            jax.ShapeDtypeStruct((tok + reach, width), BF16),
            jax.ShapeDtypeStruct((own_rows, width), F32),
            jax.ShapeDtypeStruct(gate_slabs.shape, BF16),
            jax.ShapeDtypeStruct(up_slabs.shape, BF16),
            jax.ShapeDtypeStruct(down_slabs.shape, BF16),
        ),
        in_specs=[near] * 7 + [far] * 3,
        out_specs=(near, near, far, far, far),
        scratch_shapes=buffers + semaphores,
        compiler_params=pltpu.CompilerParams(
            collective_id=0, has_side_effects=True, vmem_limit_bytes=VMEM_BYTES
        ),
        cost_estimate=pl.CostEstimate(
            flops=16 * slots * 2 * width * hidden, bytes_accessed=60_000_000, transcendentals=0
        ),
    )(
        conv_out,
        ln_gain[None],
        proj_weight,
        stream_mid,
        out_grad,
        routes.T,
        route_probs.T,
        gate_slabs,
        up_slabs,
        down_slabs,
    )
    whole = [pltpu.VMEM(x.shape[1:], BF16) for x in (gate, up, down)]
    return pl.pallas_call(
        finish_kernel,
        out_shape=(
            jax.ShapeDtypeStruct((tok, width), BF16),
            jax.ShapeDtypeStruct(proj.shape, F32),
            jax.ShapeDtypeStruct(gate.shape, BF16),
            jax.ShapeDtypeStruct(up.shape, BF16),
            jax.ShapeDtypeStruct(down.shape, BF16),
        ),
        in_specs=[far] * 6,
        out_specs=(near, far, far, far, far),
        scratch_shapes=whole
        + [
            vmem(ext.shape, BF16),
            vmem(taps.shape, BF16),
            vmem(proj.shape, F32),
            vmem(ext.shape, F32),
            vmem(taps.shape, F32),
            dma((3, CHUNKS)),
            dma((3, CHUNKS)),
            dma((4,)),
        ],
        compiler_params=pltpu.CompilerParams(vmem_limit_bytes=VMEM_BYTES),
        cost_estimate=pl.CostEstimate(
            flops=2 * taps.shape[0] * tok * width, bytes_accessed=22_000_000, transcendentals=0
        ),
    )(ext, taps, proj, gate, up, down)


def solution(mesh):
    return jax.shard_map(
        on_device,
        mesh=mesh,
        in_specs=(
            P("sp", "tp"),
            P("tp"),
            P(None, "tp"),
            P("sp", "tp"),
            P("sp", "tp"),
            P("sp", "tp"),
            P("sp", None),
            P("sp", None),
            P("sp", None, "tp"),
            P("sp", None, "tp"),
            P("sp", "tp", None),
        ),
        out_specs=(
            P("sp", "tp"),
            P("sp", "tp"),
            P("sp", None, "tp"),
            P("sp", None, "tp"),
            P("sp", "tp", None),
        ),
        check_vma=False,
    )
```
